256 devices in a mesh: rep: 2 (over z_hi), fs: 16 (over z_lo, x), tp: 8 (over y, core).
Axes of the slice: x: 4, y: 4, z: 8 (z_hi: 2, z_lo: 4; z = z_hi * 4 + z_lo), core: 2. Of those that a mesh axis runs over, the one named last changes fastest.
Arguments:
- tokens: bfloat16 [4096, 4096], P(('rep', 'fs'), 'tp'), may hold values from -6 to 6
- mixer_gain: float32 [4096], replicated, may hold values from 0.75 to 1.25
- gate_proj: bfloat16 [4096, 2048], P('fs', 'tp'), may hold values from -0.09375 to 0.09375
- value_proj: bfloat16 [4096, 2048], P('fs', 'tp'), may hold values from -0.09375 to 0.09375
- value_gain: float32 [16, 128], P('tp'), may hold values from 0.75 to 1.25
- spatial_mix: bfloat16 [16, 128, 128], P('tp', 'fs'), may hold values from -0.5 to 0.5
- spatial_bias: float32 [16, 128], P('tp'), may hold values from 0.5 to 1.5
- head_gain: float32 [16, 128], P('tp'), may hold values from 0.75 to 1.25
- merge_proj: bfloat16 [2048, 4096], P('tp', 'fs'), may hold values from -0.125 to 0.125
- ffn_gain: float32 [4096], replicated, may hold values from 0.25 to 1.75
- gate_up: bfloat16 [4096, 11008], P('fs', 'tp'), may hold values from -0.09375 to 0.09375
- value_up: bfloat16 [4096, 11008], P('fs', 'tp'), may hold values from -0.09375 to 0.09375
- gate_kernel: float32 [3, 11008], P(None, 'tp'), may hold values from -3.5 to 3.5
- value_kernel: float32 [3, 11008], P(None, 'tp'), may hold values from -3.5 to 3.5
- gate_offset: float32 [11008], P('tp'), may hold values from -0.6 to 0.6
- value_offset: float32 [11008], P('tp'), may hold values from -1.8 to 1.8
- down_proj: bfloat16 [11008, 4096], P('tp', 'fs'), may hold values from -0.0546875 to 0.0546875
Outputs:
- layer_out: bfloat16 [4096, 4096], P(('rep', 'fs'), 'tp')
The draws below stay inside these ranges and needn't reach their ends.
All inputs are finite; a program needn't handle non-finite values.
Results may differ from the reference program's by a relative error of at most 0.02.
Values may be sent and summed in bfloat16 or wider, within the bound.
No kernel may reach another device: no remote copies, remote signals or barrier semaphores. Data moves between devices by JAX's collectives and lax.ppermute only.
A program may use at most 128 MiB of HBM per device.

```python
import jax
import jax.numpy as jnp
from jax import lax

D = 4096
HEADS = 16
HEAD_DIM = 128
SEQ_LEN = 128
FF = 11008
DG = 2048
TOKENS = 4096


def shard_levels(own_key, extent, shards, smallest, top_value):
    level = 1.0
    for axis_at, blocks in shards:
        steps = jax.random.uniform(jax.random.fold_in(jax.random.fold_in(own_key, 6), axis_at), (blocks,), jnp.float32, smallest / len(shards), top_value / len(shards))
        level = level * jnp.repeat(jnp.exp(steps), extent[axis_at] // blocks).reshape((-1,) + (1,) * (len(extent) - 1 - axis_at))
    return level


def scatter_about(own_key, shape, deviation, bound, cuts=(), dtype=jnp.bfloat16):
    drawn = deviation * jax.random.normal(own_key, shape, jnp.float32)
    if cuts:
        drawn = drawn * shard_levels(own_key, shape, cuts, -0.22, 0.18)
    return jnp.clip(drawn, -bound, bound).astype(dtype)


def setup_inputs(seed: int = 0) -> dict:
    keys = jax.random.split(jax.random.key(seed), 18)
    tokens = scatter_about(keys[0], (TOKENS, D), 1.0, 6.0, ((0, 32), (1, 8)))
    mixer_gain = jnp.clip(1.0 + 0.05 * jax.random.normal(keys[1], (D,), jnp.float32), 0.75, 1.25)
    gate_proj = scatter_about(keys[2], (D, DG), D ** -0.5, 0.09375, ((0, 16), (1, 8)))
    value_proj = scatter_about(keys[3], (D, DG), D ** -0.5, 0.09375, ((0, 16), (1, 8)))
    value_gain = jnp.clip(1.0 + 0.05 * jax.random.normal(keys[4], (HEADS, HEAD_DIM), jnp.float32), 0.75, 1.25)
    spatial_mix = scatter_about(keys[5], (HEADS, SEQ_LEN, SEQ_LEN), SEQ_LEN ** -0.5, 0.5, ((0, 8), (1, 16)))
    spatial_bias = jnp.clip(1.0 + 0.1 * jax.random.normal(keys[6], (HEADS, SEQ_LEN), jnp.float32), 0.5, 1.5)
    head_gain = jnp.clip(1.0 + 0.05 * jax.random.normal(keys[7], (HEADS, HEAD_DIM), jnp.float32), 0.75, 1.25)
    merge_proj = scatter_about(keys[8], (DG, D), DG ** -0.5, 0.125, ((0, 8), (1, 16)))
    ffn_gain = jnp.clip(1.0 + 0.15 * jax.random.normal(keys[9], (D,), jnp.float32), 0.25, 1.75)
    gate_up = scatter_about(keys[10], (D, FF), D ** -0.5, 0.09375, ((0, 16), (1, 8)))
    value_up = scatter_about(keys[11], (D, FF), D ** -0.5, 0.09375, ((0, 16), (1, 8)))
    gate_kernel = scatter_about(keys[12], (3, FF), 3 ** -0.5, 3.5, ((1, 8),), jnp.float32)
    value_kernel = scatter_about(keys[13], (3, FF), 3 ** -0.5, 3.5, ((1, 8),), jnp.float32)
    gate_offset = scatter_about(keys[14], (FF,), 0.1, 0.6, ((0, 8),), jnp.float32)
    value_offset = scatter_about(keys[15], (FF,), 0.3, 1.8, ((0, 8),), jnp.float32)
    down_proj = scatter_about(keys[16], (FF, D), FF ** -0.5, 0.0546875, ((0, 8), (1, 16)))
    return {"tokens": tokens, "mixer_gain": mixer_gain, "gate_proj": gate_proj, "value_proj": value_proj, "value_gain": value_gain, "spatial_mix": spatial_mix, "spatial_bias": spatial_bias, "head_gain": head_gain, "merge_proj": merge_proj, "ffn_gain": ffn_gain, "gate_up": gate_up, "value_up": value_up, "gate_kernel": gate_kernel, "value_kernel": value_kernel, "gate_offset": gate_offset, "value_offset": value_offset, "down_proj": down_proj}


epsilon = 1e-06

def normalize(values, gain):
    values = values.astype(jnp.float32)
    scaled = values * lax.rsqrt(lax.optimization_barrier(jnp.mean(values * values, axis=-1, keepdims=True)) + epsilon)
    return scaled * gain

def rounded(values):
    return lax.optimization_barrier(values.astype(jnp.bfloat16)).astype(jnp.float32)

def gelu_exact(values):
    return jax.nn.gelu(values, approximate=False)

def convolve(values, kernel, offset, length):
    total_rows, width = values.shape
    blocks = values.reshape(total_rows // length, length, width)
    padded = jnp.pad(blocks, ((0, 0), (1, 1), (0, 0)))
    result = offset + padded[:, 0:length] * kernel[0] + padded[:, 1:length + 1] * kernel[1] + padded[:, 2:] * kernel[2]
    return result.reshape(total_rows, width)

def reference(tokens, mixer_gain, gate_proj, value_proj, value_gain, spatial_mix, spatial_bias, head_gain, merge_proj, ffn_gain, gate_up, value_up, gate_kernel, value_kernel, gate_offset, value_offset, down_proj):
    total_rows = tokens.shape[0]
    seqs = total_rows // SEQ_LEN
    normed = normalize(tokens, mixer_gain).astype(jnp.bfloat16)
    gated = gelu_exact(rounded(jnp.dot(normed, gate_proj, preferred_element_type=jnp.float32)))
    spread = gelu_exact(rounded(jnp.dot(normed, value_proj, preferred_element_type=jnp.float32)))
    spread = normalize(spread.reshape(seqs, SEQ_LEN, HEADS, HEAD_DIM), value_gain).astype(jnp.bfloat16)
    mixed = jnp.einsum('hij,njhd->nihd', spatial_mix.astype(jnp.float32), spread.astype(jnp.float32), precision=lax.Precision.HIGHEST)
    mixed = mixed + spatial_bias.T[None, :, :, None]
    joined = gated.reshape(seqs, SEQ_LEN, HEADS, HEAD_DIM) * mixed
    merged = normalize(joined, head_gain).astype(jnp.bfloat16).reshape(total_rows, DG)
    branch = jnp.dot(merged, merge_proj, preferred_element_type=jnp.float32)
    hidden = (tokens.astype(jnp.float32) + branch).astype(jnp.bfloat16)
    normed_ffn = normalize(hidden, ffn_gain).astype(jnp.bfloat16)
    upper_gate = rounded(jnp.dot(normed_ffn, gate_up, preferred_element_type=jnp.float32))
    upper_value = rounded(jnp.dot(normed_ffn, value_up, preferred_element_type=jnp.float32))
    conv_gate = convolve(upper_gate, gate_kernel, gate_offset, SEQ_LEN)
    conv_value = convolve(upper_value, value_kernel, value_offset, SEQ_LEN)
    active = (gelu_exact(conv_gate) * conv_value).astype(jnp.bfloat16)
    change = jnp.dot(active, down_proj, preferred_element_type=jnp.float32)
    return (hidden.astype(jnp.float32) + change).astype(jnp.bfloat16)
```

```python
import jax
import jax.numpy as jnp
from jax import lax
from jax.sharding import Mesh
from jax.sharding import PartitionSpec as P

REP, ZLO, X, Y, CORE = "rep", "fs_0", "fs_1", "tp_0", "tp_1"
TP = (Y, CORE)
FS = (ZLO, X)
REP_FS = (REP, ZLO, X)
RING = 4
BF16 = jnp.bfloat16
F32 = jnp.float32

epsilon = 1e-06


def shift(value, axes, size, by):
    return lax.ppermute(value, axes, [(i, (i + by) % size) for i in range(size)])


def shift_x(value, by):
    return shift(value, X, RING, by)


def shift_y(value, by):
    return shift(value, Y, RING, by)


def swap_core(value):
    return shift(value, CORE, 2, 1)


def shift_z(value, by):
    return shift(value, (REP, ZLO), 2 * RING, by)


def gather_z(block, forward_up):
    above = shift_z(block, -1)
    below = shift_z(block, 1)
    far = shift_z(above, -1) if forward_up else shift_z(below, 1)
    return [block, above, far, below]


def pick(stack, index):
    return lax.dynamic_index_in_dim(stack, index, 0, keepdims=False)


def rolled_to_front(stack, start):
    return lax.dynamic_slice_in_dim(jnp.concatenate([stack, stack], 0), start, stack.shape[0], 0)


def dot(left, right):
    return jnp.dot(left, right, preferred_element_type=F32)


def two_parts(values):
    high = lax.reduce_precision(values, 8, 7)
    return jnp.stack([high, values - high], -1).astype(BF16)


def normalize(values, gain):
    scaled = values * lax.rsqrt(jnp.mean(values * values, axis=-1, keepdims=True) + epsilon)
    return scaled * gain


def gelu_exact(values):
    return jax.nn.gelu(values, approximate=False)


def body(
    tokens,
    mixer_gain,
    gate_proj,
    value_proj,
    value_gain,
    spatial_mix,
    spatial_bias,
    head_gain,
    merge_proj,
    ffn_gain,
    gate_up,
    value_up,
    gate_kernel,
    value_kernel,
    gate_offset,
    value_offset,
    down_proj,
):
    z, x, y, core = (lax.axis_index(axis) for axis in (ZLO, X, Y, CORE))
    length, features = tokens.shape
    heads, rows, _ = spatial_mix.shape
    part, width = gate_proj.shape
    inner = gate_up.shape[1]
    full = mixer_gain.shape[0]
    half = length // 2
    shards = full // part

    pack = jnp.concatenate(
        [gate_proj, value_proj, merge_proj, spatial_mix.reshape(-1, part)], 0
    )
    packs = gather_z(pack, True)
    gates = gather_z(gate_up, True)
    values = gather_z(value_up, False)
    downs = gather_z(down_proj, False)

    def own_columns(gain):
        by_block = gain.reshape(RING, RING, part)
        mine = lax.dynamic_index_in_dim(by_block, x, 1, keepdims=False)
        return rolled_to_front(mine, z).reshape(-1)

    halves = tokens.reshape(length, 2, part)
    blocks = []
    for k in range(RING):
        piece = lax.dynamic_index_in_dim(halves, (x + k) % 2, 1, keepdims=False)
        if k:
            pairs = [
                (2 * i + c, 2 * ((i + k) % RING) + c)
                for i in range(RING)
                for c in range(2)
                if (i + k) % RING // 2 == c
            ]
            piece = lax.ppermute(piece, (X, CORE), pairs)
        blocks.append(piece)
    column = jnp.concatenate(blocks, 0)
    columns = [column]
    for k in range(1, RING):
        pairs = [
            ((i * RING + j) * 2 + i // 2, (i * RING + (j + k) % RING) * 2 + i // 2)
            for i in range(RING)
            for j in range(RING)
        ]
        columns.append(lax.ppermute(column, (X, Y, CORE), pairs))
    columns = jnp.stack(columns)
    received = lax.ppermute(
        columns, (X, CORE), [(2 * i + i // 2, 2 * i + 1 - i // 2) for i in range(RING)]
    )
    columns = jnp.where(x // 2 == core, columns, received)
    raw = jnp.concatenate([pick(columns, (y - z - j) % RING) for j in range(RING)], 1)
    raw32 = raw.astype(F32)
    squares = jnp.sum(raw32 * raw32, axis=1)
    scaled = (raw32 * own_columns(mixer_gain)).astype(BF16)

    weight = jnp.concatenate([jnp.concatenate([p[:part], p[part : 2 * part]], 1) for p in packs], 0)
    partial = dot(scaled, weight).astype(BF16)
    spatial = jnp.concatenate([p[3 * part :].reshape(-1) for p in packs]).reshape(length, -1)
    extra = two_parts(squares)
    sums = 0.0
    spatials = []
    for t in range(RING):
        at = slice(t * length, (t + 1) * length)
        payload = jnp.concatenate([partial[at], spatial, extra[at]], 1)
        if t:
            payload = shift_x(payload, -t)
        spatials.append(payload[:, 2 * width : 2 * width + spatial.shape[1]])
        sums = sums + jnp.concatenate([payload[:, : 2 * width], payload[:, -2:]], 1).astype(F32)
    scale = lax.rsqrt((sums[:, -2:-1] + sums[:, -1:]) / full + epsilon)
    pre = (sums[:, : 2 * width] * scale).astype(BF16).astype(F32)
    acted = gelu_exact(pre)
    gated, spread = acted[:, :width], acted[:, width:]
    head_width = width // heads
    spread = normalize(spread.reshape(length, heads, head_width), value_gain).astype(BF16)
    matrix = jnp.stack(spatials).reshape(RING, RING, heads, rows, length)
    matrix = rolled_to_front(matrix, (RING - x) % RING).swapaxes(0, 1)
    matrix = rolled_to_front(matrix, (RING - z) % RING)
    matrix = matrix.reshape(shards, heads, rows, length).swapaxes(0, 1).reshape(heads, length, length)
    mixed = jnp.einsum("hij,jhd->ihd", matrix, spread, preferred_element_type=F32)
    mixed = mixed + spatial_bias.T[:, :, None]
    joined = gated.reshape(length, heads, head_width) * mixed
    merged = normalize(joined, head_gain).astype(BF16).reshape(length, width)

    merges = jnp.stack([merged] + [shift_x(merged, k) for k in range(1, RING)])
    merges = merges.reshape(RING, 2, half, width)
    mine = lax.dynamic_index_in_dim(merges, core, 1, keepdims=False).reshape(-1, width)
    other = lax.dynamic_index_in_dim(merges, 1 - core, 1, keepdims=False).reshape(-1, width)
    weight = jnp.concatenate([p[2 * part : 3 * part] for p in packs], 1)
    received = swap_core(dot(other, weight).astype(BF16))
    branch = (dot(mine, weight) + received.astype(F32)).reshape(RING, half, -1)
    total = pick(branch, y)
    branch = branch.astype(BF16)
    for k in range(1, RING):
        total = total + shift_y(pick(branch, (y + k) % RING), k).astype(F32)
    residual = pick(raw.reshape(2 * RING, half, -1), 2 * y + core)
    hidden = (residual.astype(F32) + total).astype(BF16)

    mine = jnp.stack([hidden] + [shift_y(hidden, k) for k in range(1, RING)])
    mine = jnp.stack([pick(mine, (y - t) % RING) for t in range(RING)])
    other = swap_core(mine)
    states = jnp.concatenate([mine, other], 1)
    states32 = states.astype(F32)
    squares = jnp.sum(states32 * states32, axis=2)
    scaled = (states32 * own_columns(ffn_gain)).astype(BF16)

    gate_weight = jnp.concatenate(gates, 0)
    value_weight = jnp.concatenate(values, 0)
    extra = two_parts(squares)
    gate_sum, value_sum = 0.0, 0.0
    for t in reversed(range(RING)):
        gate_part = jnp.concatenate([dot(scaled[t], gate_weight).astype(BF16), extra[t]], 1)
        value_part = dot(scaled[t], value_weight).astype(BF16)
        if t:
            gate_part = shift_x(gate_part, -t)
            value_part = shift_x(value_part, -t)
        gate_sum = gate_sum + gate_part.astype(F32)
        value_sum = value_sum + value_part.astype(F32)
    scale = lax.rsqrt((gate_sum[:, -2:-1] + gate_sum[:, -1:]) / full + epsilon)
    gate_sum = gate_sum[:, :inner]
    position = (lax.broadcasted_iota(jnp.int32, (length, 1), 0) + half * core) % length

    def convolve(total, kernel, offset):
        pre = (total * scale).astype(BF16).astype(F32)
        before = jnp.where(position == 0, 0.0, jnp.roll(pre, 1, 0))
        after = jnp.where(position == length - 1, 0.0, jnp.roll(pre, -1, 0))
        return offset + before * kernel[0] + pre * kernel[1] + after * kernel[2]

    conv_gate = convolve(gate_sum, gate_kernel, gate_offset)
    conv_value = convolve(value_sum, value_kernel, value_offset)
    active = (gelu_exact(conv_gate) * conv_value).astype(BF16)

    actives = jnp.stack([active] + [shift_x(active, k) for k in range(1, RING)])
    ours = actives[:, :half].reshape(-1, inner)
    other = actives[:, half:].reshape(-1, inner)
    weight = jnp.concatenate(downs, 1)
    received = swap_core(dot(other, weight).astype(BF16))
    change = dot(ours, weight) + received.astype(F32)
    change = change.reshape(-1, RING, part).swapaxes(0, 1)
    total = pick(change, (y - z) % RING)
    change = change.astype(BF16)
    for k in range(1, RING):
        total = total + shift_y(pick(change, (y + k - z) % RING), k).astype(F32)
    residual = mine.reshape(-1, RING, part).swapaxes(0, 1)
    residual = pick(residual, (y - z) % RING)
    result = (residual.astype(F32) + total).astype(BF16).reshape(RING, half, part)

    result = jnp.stack([result[0]] + [shift_x(result[t], -t) for t in range(1, RING)])
    result = rolled_to_front(result, (RING - x) % RING).reshape(2, 2, half, part)
    received = swap_core(pick(result, 1 - core))
    ordered = jnp.stack([pick(result, core), received])
    ordered = rolled_to_front(ordered, core)
    return ordered.swapaxes(1, 2).reshape(length, features)


def solution(mesh):
    finer = Mesh(
        mesh.devices.reshape(mesh.shape["rep"], RING, RING, RING, 2), (REP, ZLO, X, Y, CORE)
    )
    return jax.shard_map(
        body,
        mesh=finer,
        in_specs=(
            P(REP_FS, TP),
            P(),
            P(FS, TP),
            P(FS, TP),
            P(TP, None),
            P(TP, FS, None),
            P(TP, None),
            P(TP, None),
            P(TP, FS),
            P(),
            P(FS, TP),
            P(FS, TP),
            P(None, TP),
            P(None, TP),
            P(TP),
            P(TP),
            P(TP, FS),
        ),
        out_specs=P(REP_FS, TP),
        check_vma=False,
    )
```

```python
import jax
import jax.numpy as jnp
from jax import lax
from jax.experimental import pallas as pl
from jax.experimental.pallas import tpu as pltpu
from jax.sharding import Mesh
from jax.sharding import PartitionSpec as P

REP, ZLO, X, Y, CORE = "rep", "fs_0", "fs_1", "tp_0", "tp_1"
TP = (Y, CORE)
FS = (ZLO, X)
REP_FS = (REP, ZLO, X)
RING = 4
BF16 = jnp.bfloat16
F32 = jnp.float32
LANES = 128

epsilon = 1e-06


def shift(value, axes, size, by):
    return lax.ppermute(value, axes, [(i, (i + by) % size) for i in range(size)])


def shift_x(value, by):
    return shift(value, X, RING, by)


def shift_y(value, by):
    return shift(value, Y, RING, by)


def swap_core(value):
    return shift(value, CORE, 2, 1)


def shift_z(value, by):
    return shift(value, (REP, ZLO), 2 * RING, by)


def gather_z(block, forward_up):
    above = shift_z(block, -1)
    below = shift_z(block, 1)
    far = shift_z(above, -1) if forward_up else shift_z(below, 1)
    return [block, above, far, below]


def kernel_call(body, outs, flops=0, scratch=(), name=None):
    def run(*args):
        return pl.pallas_call(
            body,
            out_shape=[jax.ShapeDtypeStruct(*out) for out in outs],
            in_specs=[pl.BlockSpec(memory_space=pltpu.VMEM)] * len(args),
            out_specs=[pl.BlockSpec(memory_space=pltpu.VMEM)] * len(outs),
            scratch_shapes=list(scratch),
            cost_estimate=pl.CostEstimate(flops=flops, bytes_accessed=0, transcendentals=0),
            compiler_params=pltpu.CompilerParams(vmem_limit_bytes=32 << 20),
            name=name,
        )(*args)

    return run


def place():
    return tuple(lax.axis_index(axis) for axis in (ZLO, X, Y, CORE))


def dot(left, right):
    return jnp.dot(left, right, preferred_element_type=F32)


def dot_t(left, right):
    return lax.dot_general(left, right, (((1,), (1,)), ((), ())), preferred_element_type=F32)


def two_parts(values):
    high = values.astype(BF16)
    return high, (values - high.astype(F32)).astype(BF16)


def gelu_exact(values):
    return 0.5 * values * (1.0 + lax.erf(values * (0.5**0.5)))


def rms(values, gain):
    return values * lax.rsqrt(jnp.mean(values * values, axis=-1, keepdims=True) + epsilon) * gain


def pick(stack, index):
    return lax.dynamic_index_in_dim(stack, index, 0, keepdims=False)


def rolled_to_front(stack, start):
    return lax.dynamic_slice_in_dim(jnp.concatenate([stack, stack], 0), start, stack.shape[0], 0)


def body(
    tokens,
    mixer_gain,
    gate_proj,
    value_proj,
    value_gain,
    spatial_mix,
    spatial_bias,
    head_gain,
    merge_proj,
    ffn_gain,
    gate_up,
    value_up,
    gate_kernel,
    value_kernel,
    gate_offset,
    value_offset,
    down_proj,
):
    z, x, y, core = place()
    length, features = tokens.shape
    heads, rows, _ = spatial_mix.shape
    part, width = gate_proj.shape
    inner = gate_up.shape[1]
    full = mixer_gain.shape[0]
    half = length // 2
    span = RING * part
    all_rows = RING * length
    padded = -(-inner // LANES) * LANES
    extra_rows = heads * rows
    pack_rows = 3 * part + extra_rows

    even = x % 2 == 0
    left, right = tokens[:, :part], tokens[:, part:]
    near = jnp.where(even, left, right)
    far = jnp.where(even, right, left)
    blocks = [near]
    for k in range(1, RING):
        pairs = [
            (2 * i + c, 2 * ((i + k) % RING) + c)
            for i in range(RING)
            for c in range(2)
            if (i + k) % RING // 2 == c
        ]
        blocks.append(lax.ppermute(far if k % 2 else near, (X, CORE), pairs))

    def pack_body(gate, value, merge, spatial, out):
        out[0:part] = gate[...]
        out[part : 2 * part] = value[...]
        out[2 * part : 3 * part] = merge[...]
        out[3 * part :, :LANES] = spatial[...]
        out[3 * part :, LANES:] = jnp.zeros((extra_rows, part - LANES), BF16)

    (pack,) = kernel_call(pack_body, [((pack_rows, part), BF16)], name="pack")(
        gate_proj, value_proj, merge_proj, spatial_mix.reshape(extra_rows, length)
    )
    packs = gather_z(pack, True)

    column = jnp.concatenate(blocks, 0)
    column, gate_t = lax.optimization_barrier((column, gate_up.T))
    gates = gather_z(gate_t, True)
    columns = [column]
    for k in range(1, RING):
        pairs = [
            ((i * RING + j) * 2 + i // 2, (i * RING + (j + k) % RING) * 2 + i // 2)
            for i in range(RING)
            for j in range(RING)
        ]
        columns.append(lax.ppermute(column, (X, Y, CORE), pairs))
    across = [(2 * i + i // 2, 2 * i + 1 - i // 2) for i in range(RING)]
    others = [lax.ppermute(c, (X, CORE), across) for c in columns]

    def project_body(*refs):
        own, other, weights = refs[0:4], refs[4:8], refs[8:12]
        gain, raw, pays = refs[12], refs[13], refs[14:18]
        z, x, y, core = place()
        for k in range(RING):
            j = (y - z - k) % RING

            @pl.when(core == x // 2)
            def _():
                raw[j] = own[k][...]

            @pl.when(core != x // 2)
            def _():
                raw[j] = other[k][...]

        squares = jnp.zeros((all_rows, 1), F32)
        gate = jnp.zeros((all_rows, width), F32)
        value = jnp.zeros((all_rows, width), F32)
        for j in range(RING):
            block = raw[j].astype(F32)
            squares = squares + jnp.sum(block * block, axis=1, keepdims=True)
            at = RING * ((z + j) % RING) + x
            scaled = (block * gain[pl.ds(at, 1), :]).astype(BF16)
            gate = gate + dot(scaled, weights[j][0:part])
            value = value + dot(scaled, weights[j][part : 2 * part])
        for t in range(RING):
            at = slice(t * length, (t + 1) * length)
            pays[t][:, :width] = gate[at].astype(BF16)
            pays[t][:, width : 2 * width] = value[at].astype(BF16)
            for j in range(RING):
                pays[t][extra_rows * j : extra_rows * (j + 1), 2 * width :] = weights[j][
                    3 * part :, :LANES
                ]
            row = jnp.broadcast_to(squares[at], (length, length)).T
            high, low = two_parts(row)
            base = RING * extra_rows
            pays[t][base : base + 16, 2 * width :] = high[:16]
            pays[t][base + 16 : base + 32, 2 * width :] = low[:16]
            pays[t][base + 32 :, 2 * width :] = jnp.zeros((length - base - 32, LANES), BF16)

    pay_shape = ((length, 2 * width + LANES), BF16)
    raw, *pays = kernel_call(
        project_body,
        [((RING, all_rows, part), BF16)] + [pay_shape] * RING,
        flops=2 * all_rows * span * 2 * width,
        name="project",
    )(*columns, *others, *packs, mixer_gain.reshape(-1, part))
    pays = [pays[0]] + [shift_x(pays[t], -t) for t in range(1, RING)]

    def mix_body(*refs):
        pays, (value_gain, bias, head_gain), out, matrix = refs[0:4], refs[4:7], refs[7], refs[8]
        z, x, y, core = place()
        base = RING * extra_rows
        squares = jnp.zeros((1, length), F32)
        total = jnp.zeros((length, 2 * width), F32)
        for t in range(RING):
            total = total + pays[t][:, : 2 * width].astype(F32)
            squares = squares + pays[t][base : base + 16, 2 * width :].astype(F32)[0:1]
            squares = squares + pays[t][base + 16 : base + 32, 2 * width :].astype(F32)[0:1]
            for j in range(RING):
                block = pays[t][extra_rows * j : extra_rows * (j + 1), 2 * width :].astype(F32)
                at = rows * (RING * ((z + j) % RING) + (x + t) % RING)
                for h in range(heads):
                    matrix[h, pl.ds(pl.multiple_of(at, rows), rows), :] = block[
                        h * rows : (h + 1) * rows
                    ]
        scale = jnp.broadcast_to(lax.rsqrt(squares / full + epsilon), (length, length)).T
        for h in range(heads):
            at = slice(h * length, (h + 1) * length)
            gated = gelu_exact((total[:, at] * scale).astype(BF16).astype(F32))
            at = slice(width + h * length, width + (h + 1) * length)
            spread = gelu_exact((total[:, at] * scale).astype(BF16).astype(F32))
            spread = rms(spread, value_gain[h : h + 1, :]).astype(BF16)
            mixed = dot(matrix[h].astype(BF16), spread)
            mixed = mixed + jnp.broadcast_to(bias[h : h + 1, :], (length, length)).T
            joined = rms(gated * mixed, head_gain[h : h + 1, :])
            out[:, h * length : (h + 1) * length] = joined.astype(BF16)

    (merged,) = kernel_call(
        mix_body,
        [((length, width), BF16)],
        flops=1 << 22,
        scratch=[pltpu.VMEM((heads, length, length), F32)],
        name="mix",
    )(*pays, value_gain, spatial_bias, head_gain)
    merges = [merged] + [shift_x(merged, k) for k in range(1, RING)]

    value_t, merges[0] = lax.optimization_barrier((value_up.T, merges[0]))
    values = gather_z(value_t, False)

    def rows_of(refs, start):
        return jnp.concatenate([r[pl.ds(pl.multiple_of(start, half), half), :] for r in refs], 0)

    def merge_other_body(*refs):
        merges, weights, out = refs[0:4], refs[4:8], refs[8]
        core = place()[3]
        left = rows_of(merges, half * (1 - core))
        for j in range(RING):
            piece = dot(left, weights[j][2 * part : 3 * part])
            out[:, j * part : (j + 1) * part] = piece.astype(BF16)

    merge_flops = 2 * (all_rows // 2) * width * span
    (other,) = kernel_call(
        merge_other_body, [((all_rows // 2, span), BF16)], flops=merge_flops, name="merge_other"
    )(*merges, *packs)
    received = swap_core(other)

    def merge_own_body(*refs):
        merges, weights, received, raw = refs[0:4], refs[4:8], refs[8], refs[9]
        keep, sends, total = refs[10], refs[11:14], refs[14]
        z, x, y, core = place()
        left = rows_of(merges, half * core)
        for j in range(RING):
            at = slice(j * part, (j + 1) * part)
            piece = dot(left, weights[j][2 * part : 3 * part])
            total[:, at] = piece + received[:, at].astype(F32)
        mine = pl.ds(pl.multiple_of(half * y, half), half)
        tokens = pl.ds(pl.multiple_of(length * y + half * core, half), half)
        for j in range(RING):
            at = slice(j * part, (j + 1) * part)
            keep[:, at] = total[mine, at] + raw[j, tokens, :].astype(F32)
        for k in range(1, RING):
            block = pl.ds(pl.multiple_of(half * ((y + k) % RING), half), half)
            sends[k - 1][...] = total[block, :].astype(BF16)

    keep, *sends = kernel_call(
        merge_own_body,
        [((half, span), F32)] + [((half, span), BF16)] * 3,
        flops=merge_flops,
        scratch=[pltpu.VMEM((all_rows // 2, span), F32)],
        name="merge_own",
    )(*merges, *packs, received, raw)
    sums = [shift_y(sends[k - 1], k) for k in range(1, RING)]

    def hidden_body(keep, first, second, third, out):
        total = keep[...] + first[...].astype(F32) + second[...].astype(F32)
        out[...] = (total + third[...].astype(F32)).astype(BF16)

    (hidden,) = kernel_call(hidden_body, [((half, span), BF16)], name="hidden")(keep, *sums)

    mine = [hidden] + [shift_y(hidden, k) for k in range(1, RING)]
    theirs = [swap_core(block) for block in mine]
    down_t, mine[0] = lax.optimization_barrier((down_proj, mine[0]))
    downs = gather_z(down_t, False)

    def scale_body(*refs):
        mine, theirs, gain, out, parts = refs[0:4], refs[4:8], refs[8], refs[9], refs[10]
        z, x, y, core = place()
        for k in range(RING):
            t = (y - k) % RING
            for side, block in ((0, mine[k]), (1, theirs[k])):
                at = slice(side * half, (side + 1) * half)
                squares = jnp.zeros((half, 1), F32)
                for j in range(RING):
                    cols = slice(j * part, (j + 1) * part)
                    piece = block[:, cols].astype(F32)
                    squares = squares + jnp.sum(piece * piece, axis=1, keepdims=True)
                    row = gain[pl.ds(RING * ((z + j) % RING) + x, 1), :]
                    out[t, at, cols] = (piece * row).astype(BF16)
                high, low = two_parts(squares)
                lane = lax.broadcasted_iota(jnp.int32, (half, LANES), 1)
                parts[t, at] = jnp.where(
                    lane == 0,
                    jnp.broadcast_to(high.astype(F32), (half, LANES)),
                    jnp.where(lane == 1, jnp.broadcast_to(low.astype(F32), (half, LANES)), 0.0),
                )

    scaled, parts = kernel_call(
        scale_body,
        [((RING, length, span), BF16), ((RING, length, LANES), F32)],
        name="scale",
    )(*mine, *theirs, ffn_gain.reshape(-1, part))

    spare = padded - inner

    def up_dot(scaled, t, weights):
        total = dot_t(scaled[t, :, :part], weights[0][...])
        for j in range(1, RING):
            total = total + dot_t(scaled[t, :, j * part : (j + 1) * part], weights[j][...])
        return total

    def up_far_body(*refs):
        scaled, parts, gates, values, gate_out, value_out = (
            refs[0], refs[1], refs[2:6], refs[6:10], refs[10], refs[11],
        )
        gate_out[:, :inner] = up_dot(scaled, 2, gates).astype(BF16)
        gate_out[:, inner:] = parts[2, :, :spare].astype(BF16)
        value_out[...] = up_dot(scaled, 2, values).astype(BF16)

    up_flops = 2 * length * span * inner
    gate_shape, value_shape = (length, padded), (length, inner)
    gate_far, value_far = kernel_call(
        up_far_body, [(gate_shape, BF16), (value_shape, BF16)], flops=2 * up_flops, name="up_far"
    )(scaled, parts, *gates, *values)
    gate_far = shift_x(gate_far, 1)
    value_far = shift_x(value_far, -1)

    def up_near_body(*refs):
        scaled, parts, gates, values = refs[0], refs[1], refs[2:6], refs[6:10]
        gate_out, value_out, gate_add, value_add, gate_own, value_own = refs[10:16]
        gate_out[:, :inner] = up_dot(scaled, 1, gates).astype(BF16)
        gate_out[:, inner:] = parts[1, :, :spare].astype(BF16)
        value_out[...] = up_dot(scaled, 3, values).astype(BF16)
        gate_add[:, :inner] = up_dot(scaled, 3, gates)
        gate_add[:, inner:] = parts[3, :, :spare]
        value_add[...] = up_dot(scaled, 1, values)
        gate_own[:, :inner] = up_dot(scaled, 0, gates)
        gate_own[:, inner:] = parts[0, :, :spare]
        value_own[...] = up_dot(scaled, 0, values)

    gate_near, value_near, gate_add, value_add, gate_own, value_own = kernel_call(
        up_near_body,
        [(gate_shape, BF16), (value_shape, BF16)] + [(gate_shape, F32), (value_shape, F32)] * 2,
        flops=6 * up_flops,
        name="up_near",
    )(scaled, parts, *gates, *values)
    gate_near = shift_x(gate_near, -1)
    value_near = shift_x(value_near, 1)

    def joined_gate(first, second, out):
        total = first + second
        out[...] = total.astype(BF16)
        squares = total[:, inner : inner + 1] + total[:, inner + 1 : inner + 2]
        high, low = two_parts(squares)
        out[:, inner : inner + 1] = high
        out[:, inner + 1 : inner + 2] = low

    def up_join_body(gate_far, value_far, gate_add, value_add, gate_out, value_out):
        joined_gate(gate_far[...].astype(F32), gate_add[...], gate_out)
        value_out[...] = (value_far[...].astype(F32) + value_add[...]).astype(BF16)

    gate_join, value_join = kernel_call(
        up_join_body, [(gate_shape, BF16), (value_shape, BF16)], name="up_join"
    )(gate_far, value_far, gate_add, value_add)
    gate_join = shift_x(gate_join, 1)
    value_join = shift_x(value_join, -1)

    def active_body(
        gate_own, gate_near, gate_join, value_own, value_near, value_join,
        gate_kernel, value_kernel, gate_offset, value_offset, out,
    ):
        core = place()[3]
        gate = gate_own[...] + gate_near[...].astype(F32) + gate_join[...].astype(F32)
        value = value_own[...] + value_near[...].astype(F32) + value_join[...].astype(F32)
        squares = gate[:, inner : inner + 1] + gate[:, inner + 1 : inner + 2]
        scale = lax.rsqrt(squares / full + epsilon)
        row = lax.broadcasted_iota(jnp.int32, (length, 1), 0)
        position = (row + half * core) % length

        def convolve(total, kernel, offset):
            pre = (total * scale).astype(BF16).astype(F32)
            before = jnp.where(position == 0, 0.0, pltpu.roll(pre, 1, 0))
            after = jnp.where(position == length - 1, 0.0, pltpu.roll(pre, length - 1, 0))
            return offset[...] + before * kernel[0:1] + pre * kernel[1:2] + after * kernel[2:3]

        conv_gate = convolve(gate[:, :inner], gate_kernel, gate_offset)
        conv_value = convolve(value, value_kernel, value_offset)
        out[...] = (gelu_exact(conv_gate) * conv_value).astype(BF16)

    (active,) = kernel_call(active_body, [((length, inner), BF16)], flops=1 << 24, name="active")(
        gate_own, gate_near, gate_join, value_own, value_near, value_join,
        gate_kernel, value_kernel, gate_offset[None], value_offset[None],
    )
    actives = [active] + [shift_x(active, k) for k in range(1, RING)]

    def down_other_body(*refs):
        actives, weights, out = refs[0:4], refs[4:8], refs[8]
        left = jnp.concatenate([a[half:, :] for a in actives], 0)
        for j in range(RING):
            out[:, j * part : (j + 1) * part] = dot(left, weights[j][...]).astype(BF16)

    down_flops = 2 * (all_rows // 2) * inner * span
    (other,) = kernel_call(
        down_other_body, [((all_rows // 2, span), BF16)], flops=down_flops, name="down_other"
    )(*actives, *downs)
    received = swap_core(other)

    def down_own_body(*refs):
        actives, weights, received, mine = refs[0:4], refs[4:8], refs[8], refs[9:13]
        keep, sends, total = refs[13], refs[14:17], refs[17]
        z, x, y, core = place()
        left = jnp.concatenate([a[:half, :] for a in actives], 0)
        for j in range(RING):
            piece = dot(left, weights[j][...])
            total[j] = piece + received[:, j * part : (j + 1) * part].astype(F32)
        own = (y - z) % RING
        for k in range(1, RING):
            sends[k - 1][...] = total[(own + k) % RING].astype(BF16)
        keep[...] = total[own]
        for k in range(RING):
            at = pl.ds(pl.multiple_of(half * ((y - k) % RING), half), half)
            for j in range(RING):

                @pl.when(own == j)
                def _():
                    keep[at, :] = keep[at, :] + mine[k][:, j * part : (j + 1) * part].astype(F32)

    keep, *sends = kernel_call(
        down_own_body,
        [((all_rows // 2, part), F32)] + [((all_rows // 2, part), BF16)] * 3,
        flops=down_flops,
        scratch=[pltpu.VMEM((RING, all_rows // 2, part), F32)],
        name="down_own",
    )(*actives, *downs, received, *mine)
    sums = [shift_y(sends[k - 1], k) for k in range(1, RING)]

    def result_body(keep, first, second, third, *outs):
        total = keep[...] + first[...].astype(F32) + second[...].astype(F32)
        total = (total + third[...].astype(F32)).astype(BF16)
        for t in range(RING):
            outs[t][...] = total[t * half : (t + 1) * half]

    result = kernel_call(result_body, [((half, part), BF16)] * RING, name="result")(keep, *sums)

    result = jnp.stack([result[0]] + [shift_x(result[t], -t) for t in range(1, RING)])
    result = rolled_to_front(result, (RING - x) % RING).reshape(2, 2, half, part)
    received = swap_core(pick(result, 1 - core))
    ordered = jnp.stack([pick(result, core), received])
    ordered = rolled_to_front(ordered, core)
    return ordered.swapaxes(1, 2).reshape(length, features)


def solution(mesh):
    finer = Mesh(
        mesh.devices.reshape(mesh.shape["rep"], RING, RING, RING, 2), (REP, ZLO, X, Y, CORE)
    )
    return jax.shard_map(
        body,
        mesh=finer,
        in_specs=(
            P(REP_FS, TP),
            P(),
            P(FS, TP),
            P(FS, TP),
            P(TP, None),
            P(TP, FS, None),
            P(TP, None),
            P(TP, None),
            P(TP, FS),
            P(),
            P(FS, TP),
            P(FS, TP),
            P(None, TP),
            P(None, TP),
            P(TP),
            P(TP),
            P(TP, FS),
        ),
        out_specs=P(REP_FS, TP),
        check_vma=False,
    )
```

```python
import jax
import jax.numpy as jnp
from jax import lax
from jax.experimental import pallas as pl
from jax.experimental.pallas import tpu as pltpu
from jax.sharding import Mesh
from jax.sharding import PartitionSpec as P


REP, ZLO, X, Y, CORE = "rep", "fs_0", "fs_1", "tp_0", "tp_1"
TP = (Y, CORE)
FS = (ZLO, X)
REP_FS = (REP, ZLO, X)
RING = 4
BF16 = jnp.bfloat16
F32 = jnp.float32
LANES = 128

epsilon = 1e-06


def shift(value, axes, size, by):
    return lax.ppermute(value, axes, [(i, (i + by) % size) for i in range(size)])


def shift_x(value, by):
    return shift(value, X, RING, by)


def shift_y(value, by):
    return shift(value, Y, RING, by)


def swap_core(value):
    return shift(value, CORE, 2, 1)


def shift_z(value, by):
    size = 2 * RING
    pairs = [(2 * i + c, 2 * ((i + by * (1 - 2 * c)) % size) + c) for i in range(size) for c in range(2)]
    return lax.ppermute(value, (REP, ZLO, CORE), pairs)


def gather_z(block):
    first = shift_z(block, 1)
    second = shift_z(block, -1)
    return [block, first, second, shift_z(first, 1)]


def order_z(core):
    return 0, RING - 1 - 2 * core, 1 + 2 * core, 2


def trade(value, flip):
    pairs = [
        (2 * i + c, 2 * (2 * c + (i % 2 if not flip else 1 - i % 2)) + i // 2)
        for i in range(RING)
        for c in range(2)
    ]
    return lax.ppermute(value, (X, CORE), pairs)


def kernel_call(body, outs, flops=0, scratch=(), hbm_in=(), hbm_out=(), limit=16):
    def run(*args):
        def spec(at, where):
            return pl.BlockSpec(memory_space=pltpu.HBM if at in where else pltpu.VMEM)

        return pl.pallas_call(
            body,
            out_shape=[jax.ShapeDtypeStruct(*out) for out in outs],
            in_specs=[spec(i, hbm_in) for i in range(len(args))],
            out_specs=[spec(i, hbm_out) for i in range(len(outs))],
            scratch_shapes=list(scratch),
            cost_estimate=pl.CostEstimate(flops=flops, bytes_accessed=0, transcendentals=0),
            compiler_params=pltpu.CompilerParams(vmem_limit_bytes=limit << 20),
        )(*args)

    return run


def place():
    return tuple(lax.axis_index(axis) for axis in (ZLO, X, Y, CORE))


def aligned(start, size):
    return pl.ds(pl.multiple_of(start, size), size)


def dot(left, right):
    return jnp.dot(left, right, preferred_element_type=F32)


def dot_t(left, right):
    return lax.dot_general(left, right, (((1,), (1,)), ((), ())), preferred_element_type=F32)


def two_parts(values):
    high = values.astype(BF16)
    return high, (values - high.astype(F32)).astype(BF16)


def gelu_exact(values):
    return 0.5 * values * (1.0 + lax.erf(values * (0.5**0.5)))


def rms(values, gain):
    return values * lax.rsqrt(jnp.mean(values * values, axis=-1, keepdims=True) + epsilon) * gain


def body(
    tokens,
    mixer_gain,
    gate_proj,
    value_proj,
    value_gain,
    spatial_mix,
    spatial_bias,
    head_gain,
    merge_proj,
    ffn_gain,
    gate_up,
    value_up,
    gate_kernel,
    value_kernel,
    gate_offset,
    value_offset,
    down_proj,
):
    length, features = tokens.shape
    heads, rows, _ = spatial_mix.shape
    part, width = gate_proj.shape
    inner = gate_up.shape[1]
    full = mixer_gain.shape[0]
    half = length // 2
    span = RING * part
    all_rows = RING * length
    own_rows = 2 * length
    padded = -(-inner // LANES) * LANES
    extra_rows = heads * rows
    pack_rows = 3 * part + extra_rows

    def turn(x, xs):
        return (x - xs) % RING

    def entry_body(tokens, near, far):
        x = place()[1]
        near[...] = tokens[:, aligned(part * (x % 2), part)]
        far[...] = tokens[:, aligned(part * (1 - x % 2), part)]

    piece = ((length, part), BF16)
    near, far = kernel_call(entry_body, [piece, piece])(tokens)
    near, far = trade(near, False), trade(far, True)

    def pack_body(gate, value, merge, spatial, pack):
        pack[0:part] = gate[...]
        pack[part : 2 * part] = value[...]
        pack[2 * part : 3 * part] = merge[...]
        pack[3 * part :, :LANES] = spatial[...]
        pack[3 * part :, LANES:] = jnp.zeros((extra_rows, part - LANES), BF16)

    (pack,) = kernel_call(pack_body, [((pack_rows, part), BF16)])(
        gate_proj, value_proj, merge_proj, spatial_mix.reshape(extra_rows, length)
    )
    packs = gather_z(pack)
    gates = gather_z(gate_up.T)
    values = gather_z(value_up.T)
    downs = gather_z(down_proj)

    def column_body(near, far, out):
        out[0:length] = near[...]
        out[length:] = far[...]

    (column,) = kernel_call(column_body, [((own_rows, part), BF16)])(near, far)
    columns = [column] + [shift_y(column, k) for k in range(1, RING)]

    def stack_body(*refs):
        for k in range(RING):
            refs[RING][k] = refs[k][...]

    (own,) = kernel_call(stack_body, [((RING, own_rows, part), BF16)])(*columns)
    other = swap_core(own)

    def project_body(*refs):
        own, other, weights = refs[0], refs[1], refs[2:6]
        gain, raw, pays = refs[6], refs[7], refs[8:12]
        z, x, y, core = place()
        for k in range(RING):
            j = (y - z - k) % RING
            for side, blocks in ((core, own), (1 - core, other)):
                for i in range(2):
                    xs = 2 * side + (x + i) % 2
                    raw[j, aligned(length * turn(x, xs), length), :] = blocks[
                        k, i * length : (i + 1) * length
                    ]
        squares = jnp.zeros((all_rows, 1), F32)
        gate = jnp.zeros((all_rows, width), F32)
        value = jnp.zeros((all_rows, width), F32)
        for j, weight in zip(order_z(core), weights):
            block = raw[j].astype(F32)
            squares = squares + jnp.sum(block * block, axis=1, keepdims=True)
            at = RING * ((z + j) % RING) + x
            scaled = (block * gain[pl.ds(at, 1), :]).astype(BF16)
            gate = gate + dot(scaled, weight[0:part])
            value = value + dot(scaled, weight[part : 2 * part])
        for t in range(RING):
            at = slice(t * length, (t + 1) * length)
            pays[t][:, :width] = gate[at].astype(BF16)
            pays[t][:, width : 2 * width] = value[at].astype(BF16)
            for j in range(RING):
                pays[t][extra_rows * j : extra_rows * (j + 1), 2 * width :] = weights[j][
                    3 * part :, :LANES
                ]
            row = jnp.broadcast_to(squares[at], (length, length)).T
            high, low = two_parts(row)
            base = RING * extra_rows
            pays[t][base : base + 16, 2 * width :] = high[:16]
            pays[t][base + 16 : base + 32, 2 * width :] = low[:16]
            pays[t][base + 32 :, 2 * width :] = jnp.zeros((length - base - 32, LANES), BF16)

    pay_shape = ((length, 2 * width + LANES), BF16)
    raw, *pays = kernel_call(
        project_body,
        [((RING, all_rows, part), BF16)] + [pay_shape] * RING,
        flops=2 * all_rows * span * 2 * width,
    )(own, other, *packs, mixer_gain.reshape(-1, part))
    pays = [pays[0]] + [shift_x(pays[t], -t) for t in range(1, RING)]

    def mix_body(*refs):
        pays, (value_gain, bias, head_gain), out, matrix = refs[0:4], refs[4:7], refs[7], refs[8]
        z, x, _, core = place()
        base = RING * extra_rows
        squares = jnp.zeros((1, length), F32)
        total = jnp.zeros((length, 2 * width), F32)
        for t in range(RING):
            total = total + pays[t][:, : 2 * width].astype(F32)
            squares = squares + pays[t][base : base + 16, 2 * width :].astype(F32)[0:1]
            squares = squares + pays[t][base + 16 : base + 32, 2 * width :].astype(F32)[0:1]
            for i, j in enumerate(order_z(core)):
                block = pays[t][extra_rows * i : extra_rows * (i + 1), 2 * width :].astype(F32)
                at = rows * (RING * ((z + j) % RING) + (x + t) % RING)
                for h in range(heads):
                    matrix[h, aligned(at, rows), :] = block[h * rows : (h + 1) * rows]
        scale = jnp.broadcast_to(lax.rsqrt(squares / full + epsilon), (length, length)).T
        for h in range(heads):
            at = slice(h * length, (h + 1) * length)
            gated = gelu_exact((total[:, at] * scale).astype(BF16).astype(F32))
            at = slice(width + h * length, width + (h + 1) * length)
            spread = gelu_exact((total[:, at] * scale).astype(BF16).astype(F32))
            spread = rms(spread, value_gain[h : h + 1, :]).astype(BF16)
            mixed = dot(matrix[h].astype(BF16), spread)
            mixed = mixed + jnp.broadcast_to(bias[h : h + 1, :], (length, length)).T
            joined = rms(gated * mixed, head_gain[h : h + 1, :])
            out[:, h * length : (h + 1) * length] = joined.astype(BF16)

    (merged,) = kernel_call(
        mix_body,
        [((length, width), BF16)],
        flops=1 << 22,
        scratch=[pltpu.VMEM((heads, length, length), F32)],
    )(*pays, value_gain, spatial_bias, head_gain)
    merges = [merged] + [shift_x(merged, k) for k in range(1, RING)]

    def side_of(blocks, scratch, x, side):
        for t in range(RING):
            scratch[t] = blocks[t][...]
        return jnp.concatenate([scratch[turn(x, 2 * side + i)] for i in range(2)], 0)

    def merge_other_body(*refs):
        merges, weights, out, blocks = refs[0:4], refs[4:8], refs[8], refs[9]
        _, x, _, core = place()
        left = side_of(merges, blocks, x, 1 - core)
        for j, weight in zip(order_z(core), weights):
            out[:, aligned(j * part, part)] = dot(left, weight[2 * part : 3 * part]).astype(BF16)

    merge_flops = 2 * own_rows * width * span
    merge_scratch = pltpu.VMEM((RING, length, width), BF16)
    (other,) = kernel_call(
        merge_other_body, [((own_rows, span), BF16)], flops=merge_flops, scratch=[merge_scratch]
    )(*merges, *packs)
    received = swap_core(other)

    def merge_own_body(*refs):
        merges, weights, received, raw = refs[0:4], refs[4:8], refs[8], refs[9]
        keep, sends, total, blocks = refs[10], refs[11:14], refs[14], refs[15]
        _, x, y, core = place()
        left = side_of(merges, blocks, x, core)
        for j, weight in zip(order_z(core), weights):
            at = aligned(j * part, part)
            total[:, at] = dot(left, weight[2 * part : 3 * part]) + received[:, at].astype(F32)
        mine = aligned(half * y, half)
        tokens = aligned(length * turn(x, 2 * core + y // 2) + half * (y % 2), half)
        for j in range(RING):
            at = slice(j * part, (j + 1) * part)
            keep[:, at] = total[mine, at] + raw[j, tokens, :].astype(F32)
        for k in range(1, RING):
            sends[k - 1][...] = total[aligned(half * ((y + k) % RING), half), :].astype(BF16)

    keep, *sends = kernel_call(
        merge_own_body,
        [((half, span), F32)] + [((half, span), BF16)] * 3,
        flops=merge_flops,
        scratch=[pltpu.VMEM((own_rows, span), F32), merge_scratch],
    )(*merges, *packs, received, raw)
    sums = [shift_y(sends[k - 1], k) for k in range(1, RING)]

    def hidden_body(keep, first, second, third, out):
        total = keep[...] + first[...].astype(F32) + second[...].astype(F32)
        out[...] = (total + third[...].astype(F32)).astype(BF16)

    (hidden,) = kernel_call(hidden_body, [((half, span), BF16)])(keep, *sums)

    mine = [hidden] + [shift_y(hidden, k) for k in range(1, RING)]
    (mine,) = kernel_call(stack_body, [((RING, half, span), BF16)])(*mine)
    theirs = swap_core(mine)

    spare = padded - inner

    def over_tiles(run):
        def step(n, carry):
            run(aligned(n * part, part))
            return carry

        lax.fori_loop(0, inner // part, step, 0)
        run(slice(inner // part * part, inner))

    def load(weights, out, sems):
        copies = []
        for i, j in enumerate(order_z(place()[3])):
            at = aligned(j * part, part)
            copies.append(pltpu.make_async_copy(weights[i], out.at[:, at], sems.at[i]))
        for copy in copies:
            copy.start()
        return copies

    def gate_load_body(*refs):
        for copy in load(refs[0:4], refs[4], refs[5]):
            copy.wait()

    load_sems = pltpu.SemaphoreType.DMA((RING,))
    (gate_all,) = kernel_call(
        gate_load_body, [((inner, span), BF16)], scratch=[load_sems], hbm_in=range(4)
    )(*gates)

    def up_far_body(*refs):
        mine, theirs, gain, gate_all, values = refs[0], refs[1], refs[2], refs[3], refs[4:8]
        gate_out, value_out, scaled, parts, value_all, sems = refs[8:14]
        z, x, y, core = place()
        copies = load(values, value_all, sems)
        lane = lax.broadcasted_iota(jnp.int32, (half, LANES), 1)
        for k in range(RING):
            ys = (y - k) % RING
            at = aligned(half * (ys % 2), half)
            for side, block in ((core, mine), (1 - core, theirs)):
                t = turn(x, 2 * side + ys // 2)
                slot = jnp.where(t == 0, 3, jnp.where(t == 2, 0, (t + 1) // 2))
                squares = jnp.zeros((half, 1), F32)
                for j in range(RING):
                    cols = slice(j * part, (j + 1) * part)
                    piece = block[k, :, cols].astype(F32)
                    squares = squares + jnp.sum(piece * piece, axis=1, keepdims=True)
                    row = gain[pl.ds(RING * ((z + j) % RING) + x, 1), :]
                    scaled[slot, at, cols] = (piece * row).astype(BF16)
                high, low = two_parts(squares)
                high = jnp.broadcast_to(high.astype(F32), (half, LANES))
                low = jnp.broadcast_to(low.astype(F32), (half, LANES))
                parts[slot, at] = jnp.where(lane == 0, high, jnp.where(lane == 1, low, 0.0))
        for copy in copies:
            copy.wait()

        def run(at):
            gate_out[:, at] = dot_t(scaled[0], gate_all[at]).astype(BF16)
            value_out[:, at] = dot_t(scaled[0], value_all[at]).astype(BF16)

        over_tiles(run)
        gate_out[:, inner:] = parts[0, :, :spare].astype(BF16)

    up_flops = 2 * length * span * inner
    gate_shape, value_shape, weight_shape = (length, padded), (length, inner), (inner, span)
    gate_two, value_two, scaled, parts, value_all = kernel_call(
        up_far_body,
        [
            (gate_shape, BF16),
            (value_shape, BF16),
            ((RING, length, span), BF16),
            ((RING, length, LANES), F32),
            (weight_shape, BF16),
        ],
        flops=2 * up_flops,
        scratch=[load_sems],
        hbm_in=range(4, 8),
        limit=24,
    )(mine, theirs, ffn_gain.reshape(-1, part), gate_all, *values)
    gate_two = shift_x(gate_two, 1)
    value_two = shift_x(value_two, -1)

    def up_near_body(scaled, parts, gates, values, *outs):
        gate_out, value_out, gate_add, value_add, gate_own, value_own = outs
        left = scaled[1:RING].reshape((RING - 1) * length, span)

        def run(at):
            piece = dot_t(left, gates[at])
            gate_out[:, at] = piece[:length].astype(BF16)
            gate_add[:, at] = piece[length : 2 * length]
            gate_own[:, at] = piece[2 * length :]
            piece = dot_t(left, values[at])
            value_add[:, at] = piece[:length]
            value_out[:, at] = piece[length : 2 * length].astype(BF16)
            value_own[:, at] = piece[2 * length :]

        over_tiles(run)
        gate_out[:, inner:] = parts[1, :, :spare].astype(BF16)
        gate_add[:, inner:] = parts[2, :, :spare]
        gate_own[:, inner:] = parts[3, :, :spare]

    gate_near, value_near, gate_add, value_add, gate_own, value_own = kernel_call(
        up_near_body,
        [(gate_shape, BF16), (value_shape, BF16)] + [(gate_shape, F32), (value_shape, F32)] * 2,
        flops=6 * up_flops,
        limit=24,
    )(scaled, parts, gate_all, value_all)
    gate_near = shift_x(gate_near, -1)
    value_near = shift_x(value_near, 1)

    def up_join_body(gate_two, value_two, gate_add, value_add, gate_out, value_out):
        total = gate_two[...].astype(F32) + gate_add[...]
        gate_out[...] = total.astype(BF16)
        squares = total[:, inner : inner + 1] + total[:, inner + 1 : inner + 2]
        high, low = two_parts(squares)
        gate_out[:, inner : inner + 1] = high
        gate_out[:, inner + 1 : inner + 2] = low
        value_out[...] = (value_two[...].astype(F32) + value_add[...]).astype(BF16)

    gate_join, value_join = kernel_call(
        up_join_body, [(gate_shape, BF16), (value_shape, BF16)]
    )(gate_two, value_two, gate_add, value_add)
    gate_join = shift_x(gate_join, 1)
    value_join = shift_x(value_join, -1)

    def active_body(
        gate_own, gate_near, gate_join, value_own, value_near, value_join,
        gate_kernel, value_kernel, gate_offset, value_offset, out,
    ):
        gates, values = (gate_own, gate_near, gate_join), (value_own, value_near, value_join)
        squares = jnp.zeros((length, 1), F32)
        for ref in gates:
            squares = squares + ref[:, inner : inner + 1].astype(F32)
            squares = squares + ref[:, inner + 1 : inner + 2].astype(F32)
        scale = lax.rsqrt(squares / full + epsilon)

        def run(at, size):
            position = lax.broadcasted_iota(jnp.int32, (length, size), 0)

            def convolve(refs, kernel, offset):
                total = refs[0][:, at] + refs[1][:, at].astype(F32) + refs[2][:, at].astype(F32)
                pre = (total * scale).astype(BF16).astype(F32)
                before = jnp.where(position == 0, 0.0, pltpu.roll(pre, 1, 0))
                after = jnp.where(position == length - 1, 0.0, pltpu.roll(pre, length - 1, 0))
                taps = before * kernel[0:1, at] + pre * kernel[1:2, at] + after * kernel[2:3, at]
                return offset[:, at] + taps

            gate = convolve(gates, gate_kernel, gate_offset)
            value = convolve(values, value_kernel, value_offset)
            out[:, at] = (gelu_exact(gate) * value).astype(BF16)

        def step(n, carry):
            run(aligned(n * LANES, LANES), LANES)
            return carry

        lax.fori_loop(0, inner // LANES, step, 0)
        rest = inner // LANES * LANES
        run(slice(rest, inner), inner - rest)

    (active,) = kernel_call(active_body, [((length, inner), BF16)], flops=1 << 24)(
        gate_own, gate_near, gate_join, value_own, value_near, value_join,
        gate_kernel, value_kernel, gate_offset[None], value_offset[None],
    )
    actives = [active] + [shift_x(active, k) for k in range(1, RING)]

    def down_body(side_is_own):
        def run(*refs):
            actives, weights, out, blocks = refs[0:4], refs[4:8], refs[8], refs[9]
            _, x, _, core = place()
            left = side_of(actives, blocks, x, core if side_is_own else 1 - core)
            for j, weight in zip(order_z(core), weights):
                out[j] = dot(left, weight[...]).astype(out.dtype)

        return kernel_call(
            run,
            [((RING, own_rows, part), F32 if side_is_own else BF16)],
            flops=2 * own_rows * inner * span,
            scratch=[pltpu.VMEM((RING, length, inner), BF16)],
        )

    (other,) = down_body(False)(*actives, *downs)
    received = swap_core(other)
    (own,) = down_body(True)(*actives, *downs)

    def down_add_body(*refs):
        own, received, mine, keep, sends = refs[0], refs[1], refs[2], refs[3], refs[4:7]
        z, _, y, _ = place()
        at = (y - z) % RING
        for k in range(1, RING):
            j = (at + k) % RING
            sends[k - 1][...] = (own[j] + received[j].astype(F32)).astype(BF16)
        keep[...] = own[at] + received[at].astype(F32)
        for k in range(RING):
            place_rows = aligned(half * ((y - k) % RING), half)
            for j in range(RING):

                @pl.when(at == j)
                def _():
                    piece = mine[k, :, j * part : (j + 1) * part].astype(F32)
                    keep[place_rows, :] = keep[place_rows, :] + piece

    block = (own_rows, part)
    keep, *sends = kernel_call(
        down_add_body, [(block, F32)] + [(block, BF16)] * 3, flops=1 << 20
    )(own, received, mine)
    sums = [shift_y(sends[k - 1], k) for k in range(1, RING)]

    def result_body(keep, first, second, third, near, far, total):
        x = place()[1]
        added = keep[...] + first[...].astype(F32) + second[...].astype(F32)
        total[...] = added + third[...].astype(F32)
        near[...] = total[aligned(length * (x % 2), length), :].astype(BF16)
        far[...] = total[aligned(length * (1 - x % 2), length), :].astype(BF16)

    near, far = kernel_call(
        result_body, [piece, piece], scratch=[pltpu.VMEM(block, F32)]
    )(keep, *sums)

    near, far = trade(near, False), trade(far, True)

    def exit_body(near, far, out, sems):
        x = place()[1]
        moves = [
            (near, out.at[:, aligned(part * (x % 2), part)]),
            (far, out.at[:, aligned(part * (1 - x % 2), part)]),
        ]
        copies = [pltpu.make_async_copy(a, b, sems.at[i]) for i, (a, b) in enumerate(moves)]
        for copy in copies:
            copy.start()
        for copy in copies:
            copy.wait()

    (out,) = kernel_call(
        exit_body,
        [((length, features), BF16)],
        scratch=[pltpu.SemaphoreType.DMA((2,))],
        hbm_in=range(2),
        hbm_out=range(1),
    )(near, far)
    return out


def solution(mesh):
    finer = Mesh(
        mesh.devices.reshape(mesh.shape["rep"], RING, RING, RING, 2), (REP, ZLO, X, Y, CORE)
    )

    return jax.shard_map(
        body,
        mesh=finer,
        in_specs=(
            P(REP_FS, TP),
            P(),
            P(FS, TP),
            P(FS, TP),
            P(TP, None),
            P(TP, FS, None),
            P(TP, None),
            P(TP, None),
            P(TP, FS),
            P(),
            P(FS, TP),
            P(FS, TP),
            P(None, TP),
            P(None, TP),
            P(TP),
            P(TP),
            P(TP, FS),
        ),
        out_specs=P(REP_FS, TP),
        check_vma=False,
    )
```

```python
import jax
import jax.numpy as jnp
from jax import lax
from jax.experimental import pallas as pl
from jax.experimental.pallas import tpu as pltpu
from jax.sharding import Mesh
from jax.sharding import PartitionSpec as P


REP, ZLO, X, Y, CORE = "rep", "fs_0", "fs_1", "tp_0", "tp_1"
TP = (Y, CORE)
FS = (ZLO, X)
REP_FS = (REP, ZLO, X)
RING = 4
BF16 = jnp.bfloat16
F32 = jnp.float32
LANES = 128

epsilon = 1e-06


def shift(value, axes, size, by):
    return lax.ppermute(value, axes, [(i, (i + by) % size) for i in range(size)])


def shift_x(value, by):
    return shift(value, X, RING, by)


def shift_y(value, by):
    return shift(value, Y, RING, by)


def swap_core(value):
    return shift(value, CORE, 2, 1)


def shift_apart(value, axes, size, by):
    pairs = [(2 * i + c, 2 * ((i + by * (1 - 2 * c)) % size) + c) for i in range(size) for c in range(2)]
    return lax.ppermute(value, (*axes, CORE), pairs)


def gather_ring(value, axes, size):
    first = shift_apart(value, axes, size, 1)
    second = shift_apart(value, axes, size, -1)
    return [value, first, second, shift_apart(first, axes, size, 1)]


def gather_z(block):
    return gather_ring(block, (REP, ZLO), 2 * RING)


def order_before(core):
    return 0, 1 + 2 * core, RING - 1 - 2 * core, 2


def order_z(core):
    return 0, RING - 1 - 2 * core, 1 + 2 * core, 2


def trade(value, flip):
    pairs = [
        (2 * i + c, 2 * (2 * c + (i % 2 if not flip else 1 - i % 2)) + i // 2)
        for i in range(RING)
        for c in range(2)
    ]
    return lax.ppermute(value, (X, CORE), pairs)


def kernel_call(body, outs, flops=0, scratch=(), hbm_in=(), hbm_out=(), limit=16):
    def run(*args):
        def spec(at, where):
            return pl.BlockSpec(memory_space=pltpu.HBM if at in where else pltpu.VMEM)

        return pl.pallas_call(
            body,
            out_shape=[jax.ShapeDtypeStruct(*out) for out in outs],
            in_specs=[spec(i, hbm_in) for i in range(len(args))],
            out_specs=[spec(i, hbm_out) for i in range(len(outs))],
            scratch_shapes=list(scratch),
            cost_estimate=pl.CostEstimate(flops=flops, bytes_accessed=0, transcendentals=0),
            compiler_params=pltpu.CompilerParams(vmem_limit_bytes=limit << 20),
        )(*args)

    return run


def place():
    return tuple(lax.axis_index(axis) for axis in (ZLO, X, Y, CORE))


def aligned(start, size):
    return pl.ds(pl.multiple_of(start, size), size)


def dot(left, right):
    return jnp.dot(left, right, preferred_element_type=F32)


def dot_t(left, right):
    return lax.dot_general(left, right, (((1,), (1,)), ((), ())), preferred_element_type=F32)


def two_parts(values):
    high = values.astype(BF16)
    return high, (values - high.astype(F32)).astype(BF16)


def gelu_exact(values):
    return 0.5 * values * (1.0 + lax.erf(values * (0.5**0.5)))


def rms(values, gain):
    return values * lax.rsqrt(jnp.mean(values * values, axis=-1, keepdims=True) + epsilon) * gain


def body(
    tokens,
    mixer_gain,
    gate_proj,
    value_proj,
    value_gain,
    spatial_mix,
    spatial_bias,
    head_gain,
    merge_proj,
    ffn_gain,
    gate_up,
    value_up,
    gate_kernel,
    value_kernel,
    gate_offset,
    value_offset,
    down_proj,
):
    length, features = tokens.shape
    heads, rows, _ = spatial_mix.shape
    part, width = gate_proj.shape
    inner = gate_up.shape[1]
    full = mixer_gain.shape[0]
    half = length // 2
    span = RING * part
    all_rows = RING * length
    own_rows = 2 * length
    padded = -(-inner // LANES) * LANES
    extra_rows = heads * rows
    pack_rows = 3 * part + extra_rows

    def turn(x, xs):
        return (x - xs) % RING

    gains = jnp.stack([mixer_gain, ffn_gain]).reshape(-1, part)

    def move(*moves):
        *pairs, sems = moves
        copies = [pltpu.make_async_copy(a, b, sems.at[i]) for i, (a, b) in enumerate(pairs)]
        for copy in copies:
            copy.start()
        for copy in copies:
            copy.wait()

    def entry_body(tokens, gate, value, merge, spatial, near, far, pack, sems):
        x = place()[1]
        move(
            (tokens.at[:, aligned(part * (x % 2), part)], near),
            (tokens.at[:, aligned(part * (1 - x % 2), part)], far),
            (gate, pack.at[0:part]),
            (value, pack.at[part : 2 * part]),
            (merge, pack.at[2 * part : 3 * part]),
            (spatial, pack.at[3 * part : pack_rows, 0:LANES]),
            sems,
        )

    piece = ((length, part), BF16)
    near, far, pack = kernel_call(
        entry_body,
        [piece, piece, ((pack_rows, part), BF16)],
        scratch=[pltpu.SemaphoreType.DMA((6,))],
        hbm_in=range(5),
        limit=62,
    )(tokens, gate_proj, value_proj, merge_proj, spatial_mix.reshape(extra_rows, length))
    near, far = trade(near, False), trade(far, True)

    packs = gather_z(pack)

    def join_body(gate, value, out, both, sems):
        move((gate, both.at[0:inner]), (value, both.at[inner : 2 * inner]), sems)
        move((both, out), sems)

    (up,) = kernel_call(
        join_body,
        [((2 * inner, part), BF16)],
        scratch=[pltpu.VMEM((2 * inner, part), BF16), pltpu.SemaphoreType.DMA((2,))],
        hbm_in=range(2),
        hbm_out=range(1),
        limit=62,
    )(gate_up.T, value_up.T)
    ups = gather_z(up)
    downs = gather_z(down_proj)

    def column_body(near, far, out):
        out[0:length] = near[...]
        out[length:] = far[...]

    (column,) = kernel_call(column_body, [((own_rows, part), BF16)])(near, far)
    columns = gather_ring(column, (Y,), RING)

    def stack_body(*refs):
        for k in range(RING):
            refs[RING][k] = refs[k][...]

    (own,) = kernel_call(stack_body, [((RING, own_rows, part), BF16)])(*columns)
    other = swap_core(own)

    def project_body(*refs):
        own, other, weights = refs[0], refs[1], refs[2:6]
        gain, raw, pays = refs[6], refs[7], refs[8:12]
        z, x, y, core = place()
        for side, blocks in ((core, own), (1 - core, other)):
            for n, k in enumerate(order_before(side)):
                j = (y - z - k) % RING
                for i in range(2):
                    xs = 2 * side + (x + i) % 2
                    raw[j, aligned(length * turn(x, xs), length), :] = blocks[
                        n, i * length : (i + 1) * length
                    ]
        squares = jnp.zeros((all_rows, 1), F32)
        gate = jnp.zeros((all_rows, width), F32)
        value = jnp.zeros((all_rows, width), F32)
        for j, weight in zip(order_z(core), weights):
            block = raw[j].astype(F32)
            squares = squares + jnp.sum(block * block, axis=1, keepdims=True)
            at = RING * ((z + j) % RING) + x
            scaled = (block * gain[pl.ds(at, 1), :]).astype(BF16)
            gate = gate + dot(scaled, weight[0:part])
            value = value + dot(scaled, weight[part : 2 * part])
        for t in range(RING):
            at = slice(t * length, (t + 1) * length)
            pays[t][:, :width] = gate[at].astype(BF16)
            pays[t][:, width : 2 * width] = value[at].astype(BF16)
            for j in range(RING):
                pays[t][extra_rows * j : extra_rows * (j + 1), 2 * width :] = weights[j][
                    3 * part :, :LANES
                ]
            row = jnp.broadcast_to(squares[at], (length, length)).T
            high, low = two_parts(row)
            base = RING * extra_rows
            pays[t][base : base + 16, 2 * width :] = high[:16]
            pays[t][base + 16 : base + 32, 2 * width :] = low[:16]
            pays[t][base + 32 :, 2 * width :] = jnp.zeros((length - base - 32, LANES), BF16)

    pay_shape = ((length, 2 * width + LANES), BF16)
    raw, *pays = kernel_call(
        project_body,
        [((RING, all_rows, part), BF16)] + [pay_shape] * RING,
        flops=2 * all_rows * span * 2 * width,
    )(own, other, *packs, gains)
    pays = [pays[0]] + [shift_x(pays[t], -t) for t in range(1, RING)]

    def mix_body(*refs):
        pays, (value_gain, bias, head_gain), out, matrix = refs[0:4], refs[4:7], refs[7], refs[8]
        z, x, _, core = place()
        base = RING * extra_rows
        squares = jnp.zeros((1, length), F32)
        total = jnp.zeros((length, 2 * width), F32)
        for t in range(RING):
            total = total + pays[t][:, : 2 * width].astype(F32)
            squares = squares + pays[t][base : base + 16, 2 * width :].astype(F32)[0:1]
            squares = squares + pays[t][base + 16 : base + 32, 2 * width :].astype(F32)[0:1]
            for i, j in enumerate(order_z(core)):
                block = pays[t][extra_rows * i : extra_rows * (i + 1), 2 * width :].astype(F32)
                at = rows * (RING * ((z + j) % RING) + (x + t) % RING)
                for h in range(heads):
                    matrix[h, aligned(at, rows), :] = block[h * rows : (h + 1) * rows]
        scale = jnp.broadcast_to(lax.rsqrt(squares / full + epsilon), (length, length)).T
        for h in range(heads):
            at = slice(h * length, (h + 1) * length)
            gated = gelu_exact((total[:, at] * scale).astype(BF16).astype(F32))
            at = slice(width + h * length, width + (h + 1) * length)
            spread = gelu_exact((total[:, at] * scale).astype(BF16).astype(F32))
            spread = rms(spread, value_gain[h : h + 1, :]).astype(BF16)
            mixed = dot(matrix[h].astype(BF16), spread)
            mixed = mixed + jnp.broadcast_to(bias[h : h + 1, :], (length, length)).T
            joined = rms(gated * mixed, head_gain[h : h + 1, :])
            out[:, h * length : (h + 1) * length] = joined.astype(BF16)

    (merged,) = kernel_call(
        mix_body,
        [((length, width), BF16)],
        flops=1 << 22,
        scratch=[pltpu.VMEM((heads, length, length), F32)],
    )(*pays, value_gain, spatial_bias, head_gain)
    merges = gather_ring(merged, (X,), RING)

    def side_of(blocks, scratch, x, core, side):
        for t, block in zip(order_before(core), blocks):
            scratch[t] = block[...]
        return jnp.concatenate([scratch[turn(x, 2 * side + i)] for i in range(2)], 0)

    def merge_other_body(*refs):
        merges, weights, out, blocks = refs[0:4], refs[4:8], refs[8], refs[9]
        _, x, _, core = place()
        left = side_of(merges, blocks, x, core, 1 - core)
        for j, weight in zip(order_z(core), weights):
            out[:, aligned(j * part, part)] = dot(left, weight[2 * part : 3 * part]).astype(BF16)

    merge_flops = 2 * own_rows * width * span
    merge_scratch = pltpu.VMEM((RING, length, width), BF16)
    (other,) = kernel_call(
        merge_other_body, [((own_rows, span), BF16)], flops=merge_flops, scratch=[merge_scratch]
    )(*merges, *packs)
    received = swap_core(other)

    def merge_own_body(*refs):
        merges, weights, received, raw = refs[0:4], refs[4:8], refs[8], refs[9]
        keep, sends, total, blocks = refs[10], refs[11:14], refs[14], refs[15]
        _, x, y, core = place()
        left = side_of(merges, blocks, x, core, core)
        for j, weight in zip(order_z(core), weights):
            at = aligned(j * part, part)
            total[:, at] = dot(left, weight[2 * part : 3 * part]) + received[:, at].astype(F32)
        mine = aligned(half * y, half)
        tokens = aligned(length * turn(x, 2 * core + y // 2) + half * (y % 2), half)
        for j in range(RING):
            at = slice(j * part, (j + 1) * part)
            keep[:, at] = total[mine, at] + raw[j, tokens, :].astype(F32)
        for k in range(1, RING):
            sends[k - 1][...] = total[aligned(half * ((y + k) % RING), half), :].astype(BF16)

    keep, *sends = kernel_call(
        merge_own_body,
        [((half, span), F32)] + [((half, span), BF16)] * 3,
        flops=merge_flops,
        scratch=[pltpu.VMEM((own_rows, span), F32), merge_scratch],
    )(*merges, *packs, received, raw)
    sums = [shift_y(sends[k - 1], k) for k in range(1, RING)]

    def hidden_body(keep, first, second, third, out):
        total = keep[...] + first[...].astype(F32) + second[...].astype(F32)
        out[...] = (total + third[...].astype(F32)).astype(BF16)

    (hidden,) = kernel_call(hidden_body, [((half, span), BF16)])(keep, *sums)

    mine = gather_ring(hidden, (Y,), RING)
    (mine,) = kernel_call(stack_body, [((RING, half, span), BF16)])(*mine)
    theirs = swap_core(mine)

    spare = padded - inner

    def over_tiles(run):
        def step(n, carry):
            start = pl.multiple_of(n * part, part)
            run(pl.ds(start, part), pl.ds(pl.multiple_of(inner + start, 32), part))
            return carry

        lax.fori_loop(0, inner // part, step, 0)
        rest = inner // part * part
        run(slice(rest, inner), slice(inner + rest, 2 * inner))

    def up_dot(left, weights, last, at):
        split = (RING - 1) * part
        return dot_t(left[:, :split], weights[at]) + dot_t(left[:, split:], last[at])

    def load_body(gate, value, first, second, out, sems):
        move(
            (gate, out.at[0:inner, 0:part]),
            (value, out.at[inner : 2 * inner, 0:part]),
            (first, out.at[:, part : 2 * part]),
            (second, out.at[:, 2 * part : 3 * part]),
            sems,
        )

    load_sems = pltpu.SemaphoreType.DMA((RING,))
    (weights,) = kernel_call(
        load_body, [((2 * inner, 3 * part), BF16)], scratch=[load_sems], hbm_in=range(4)
    )(gate_up.T, value_up.T, ups[1], ups[2])

    def up_far_body(*refs):
        mine, theirs, gain, weights, last_in = refs[0:5]
        gate_out, value_out, scaled, parts, last, sem = refs[5:11]
        z, x, y, core = place()
        copy = pltpu.make_async_copy(last_in, last, sem.at[0])
        copy.start()
        lane = lax.broadcasted_iota(jnp.int32, (half, LANES), 1)
        for side, block in ((core, mine), (1 - core, theirs)):
            for n, k in enumerate(order_before(side)):
                ys = (y - k) % RING
                at = aligned(half * (ys % 2), half)
                t = turn(x, 2 * side + ys // 2)
                slot = jnp.where(t == 0, 3, jnp.where(t == 2, 0, (t + 1) // 2))
                squares = jnp.zeros((half, 1), F32)
                for i, j in enumerate(order_z(core)):
                    piece = block[n, :, aligned(j * part, part)].astype(F32)
                    squares = squares + jnp.sum(piece * piece, axis=1, keepdims=True)
                    row = gain[pl.ds(RING * (RING + (z + j) % RING) + x, 1), :]
                    scaled[slot, at, i * part : (i + 1) * part] = (piece * row).astype(BF16)
                high, low = two_parts(squares)
                high = jnp.broadcast_to(high.astype(F32), (half, LANES))
                low = jnp.broadcast_to(low.astype(F32), (half, LANES))
                parts[slot, at] = jnp.where(lane == 0, high, jnp.where(lane == 1, low, 0.0))
        copy.wait()

        def run(at, value_at):
            gate_out[:, at] = up_dot(scaled[0], weights, last, at).astype(BF16)
            value_out[:, at] = up_dot(scaled[0], weights, last, value_at).astype(BF16)

        over_tiles(run)
        gate_out[:, inner:] = parts[0, :, :spare].astype(BF16)

    up_flops = 2 * length * span * inner
    gate_shape, value_shape = (length, padded), (length, inner)
    gate_two, value_two, scaled, parts, last = kernel_call(
        up_far_body,
        [
            (gate_shape, BF16),
            (value_shape, BF16),
            ((RING, length, span), BF16),
            ((RING, length, LANES), F32),
            ((2 * inner, part), BF16),
        ],
        flops=2 * up_flops,
        scratch=[pltpu.SemaphoreType.DMA((1,))],
        hbm_in=range(4, 5),
        limit=24,
    )(mine, theirs, gains, weights, ups[3])
    gate_two = shift_x(gate_two, 1)
    value_two = shift_x(value_two, -1)

    def up_near_body(scaled, parts, weights, last, *outs):
        gate_out, value_out, gate_add, value_add, gate_own, value_own = outs
        left = scaled[1:RING].reshape((RING - 1) * length, span)

        def run(at, value_at):
            piece = up_dot(left, weights, last, at)
            gate_out[:, at] = piece[:length].astype(BF16)
            gate_add[:, at] = piece[length : 2 * length]
            gate_own[:, at] = piece[2 * length :]
            piece = up_dot(left, weights, last, value_at)
            value_add[:, at] = piece[:length]
            value_out[:, at] = piece[length : 2 * length].astype(BF16)
            value_own[:, at] = piece[2 * length :]

        over_tiles(run)
        gate_out[:, inner:] = parts[1, :, :spare].astype(BF16)
        gate_add[:, inner:] = parts[2, :, :spare]
        gate_own[:, inner:] = parts[3, :, :spare]

    gate_near, value_near, gate_add, value_add, gate_own, value_own = kernel_call(
        up_near_body,
        [(gate_shape, BF16), (value_shape, BF16)] + [(gate_shape, F32), (value_shape, F32)] * 2,
        flops=6 * up_flops,
        limit=24,
    )(scaled, parts, weights, last)
    gate_near = shift_x(gate_near, -1)
    value_near = shift_x(value_near, 1)

    def up_join_body(gate_two, value_two, gate_add, value_add, gate_out, value_out):
        def step(n, carry):
            at = aligned(n * 16, 16)
            gate_out[at] = (gate_two[at].astype(F32) + gate_add[at]).astype(BF16)
            value_out[at] = (value_two[at].astype(F32) + value_add[at]).astype(BF16)
            return carry

        lax.fori_loop(0, length // 16, step, 0)
        total = gate_two[:, inner:].astype(F32) + gate_add[:, inner:]
        high, low = two_parts(total[:, 0:1] + total[:, 1:2])
        gate_out[:, inner : inner + 1] = high
        gate_out[:, inner + 1 : inner + 2] = low

    gate_join, value_join = kernel_call(
        up_join_body, [(gate_shape, BF16), (value_shape, BF16)]
    )(gate_two, value_two, gate_add, value_add)
    gate_join = shift_x(gate_join, 1)
    value_join = shift_x(value_join, -1)

    def active_body(
        gate_own, gate_near, gate_join, value_own, value_near, value_join,
        gate_kernel, value_kernel, gate_offset, value_offset, out,
    ):
        gates, values = (gate_own, gate_near, gate_join), (value_own, value_near, value_join)
        squares = jnp.zeros((length, 1), F32)
        for ref in gates:
            squares = squares + ref[:, inner : inner + 1].astype(F32)
            squares = squares + ref[:, inner + 1 : inner + 2].astype(F32)
        scale = lax.rsqrt(squares / full + epsilon)

        def run(at, size):
            position = lax.broadcasted_iota(jnp.int32, (length, size), 0)

            def convolve(refs, kernel, offset):
                total = refs[0][:, at] + refs[1][:, at].astype(F32) + refs[2][:, at].astype(F32)
                pre = (total * scale).astype(BF16).astype(F32)
                before = jnp.where(position == 0, 0.0, pltpu.roll(pre, 1, 0))
                after = jnp.where(position == length - 1, 0.0, pltpu.roll(pre, length - 1, 0))
                taps = before * kernel[0:1, at] + pre * kernel[1:2, at] + after * kernel[2:3, at]
                return offset[:, at] + taps

            gate = convolve(gates, gate_kernel, gate_offset)
            value = convolve(values, value_kernel, value_offset)
            out[:, at] = (gelu_exact(gate) * value).astype(BF16)

        def step(n, carry):
            run(aligned(n * LANES, LANES), LANES)
            return carry

        lax.fori_loop(0, inner // LANES, step, 0)
        rest = inner // LANES * LANES
        run(slice(rest, inner), inner - rest)

    (active,) = kernel_call(active_body, [((length, inner), BF16)], flops=1 << 24)(
        gate_own, gate_near, gate_join, value_own, value_near, value_join,
        gate_kernel, value_kernel, gate_offset[None], value_offset[None],
    )
    actives = gather_ring(active, (X,), RING)

    def down_load_body(*refs):
        order = order_z(place()[3])
        move(*((refs[i], refs[RING].at[j]) for i, j in enumerate(order)), refs[RING + 1])

    (weights,) = kernel_call(
        down_load_body, [((RING, inner, part), BF16)], scratch=[load_sems], hbm_in=range(4)
    )(*downs)


    def down_body(side_is_own):
        def run(*refs):
            actives, weights, out, blocks, left = refs[0:4], refs[4], refs[5], refs[6], refs[7]
            _, x, _, core = place()
            left[...] = side_of(actives, blocks, x, core, core if side_is_own else 1 - core)

            def step(j, carry):
                out[j] = dot(left[...], weights[j]).astype(out.dtype)
                return carry

            lax.fori_loop(0, RING, step, 0, unroll=2)

        return kernel_call(
            run,
            [((RING, own_rows, part), F32 if side_is_own else BF16)],
            flops=2 * own_rows * inner * span,
            scratch=[pltpu.VMEM((RING, length, inner), BF16), pltpu.VMEM((own_rows, inner), BF16)],
        )

    (other,) = down_body(False)(*actives, weights)
    received = swap_core(other)
    (own,) = down_body(True)(*actives, weights)

    def down_add_body(*refs):
        own, received, mine, keep, sends = refs[0], refs[1], refs[2], refs[3], refs[4:7]
        z, _, y, core = place()
        at = (y - z) % RING
        for k in range(1, RING):
            j = (at + k) % RING
            sends[k - 1][...] = (own[j] + received[j].astype(F32)).astype(BF16)
        keep[...] = own[at] + received[at].astype(F32)
        for n, k in enumerate(order_before(core)):
            place_rows = aligned(half * ((y - k) % RING), half)
            for j in range(RING):

                @pl.when(at == j)
                def _():
                    piece = mine[n, :, j * part : (j + 1) * part].astype(F32)
                    keep[place_rows, :] = keep[place_rows, :] + piece

    block = (own_rows, part)
    keep, *sends = kernel_call(
        down_add_body, [(block, F32)] + [(block, BF16)] * 3, flops=1 << 20
    )(own, received, mine)
    sums = [shift_y(sends[k - 1], k) for k in range(1, RING)]

    def result_body(keep, first, second, third, near, far, total):
        x = place()[1]
        added = keep[...] + first[...].astype(F32) + second[...].astype(F32)
        total[...] = added + third[...].astype(F32)
        near[...] = total[aligned(length * (x % 2), length), :].astype(BF16)
        far[...] = total[aligned(length * (1 - x % 2), length), :].astype(BF16)

    near, far = kernel_call(
        result_body, [piece, piece], scratch=[pltpu.VMEM(block, F32)]
    )(keep, *sums)

    near, far = trade(near, False), trade(far, True)

    def exit_body(near, far, out, sems):
        x = place()[1]
        move(
            (near, out.at[:, aligned(part * (x % 2), part)]),
            (far, out.at[:, aligned(part * (1 - x % 2), part)]),
            sems,
        )

    (out,) = kernel_call(
        exit_body,
        [((length, features), BF16)],
        scratch=[pltpu.SemaphoreType.DMA((2,))],
        hbm_in=range(2),
        hbm_out=range(1),
    )(near, far)
    return out


def solution(mesh):
    finer = Mesh(
        mesh.devices.reshape(mesh.shape["rep"], RING, RING, RING, 2), (REP, ZLO, X, Y, CORE)
    )

    return jax.shard_map(
        body,
        mesh=finer,
        in_specs=(
            P(REP_FS, TP),
            P(),
            P(FS, TP),
            P(FS, TP),
            P(TP, None),
            P(TP, FS, None),
            P(TP, None),
            P(TP, None),
            P(TP, FS),
            P(),
            P(FS, TP),
            P(FS, TP),
            P(None, TP),
            P(None, TP),
            P(TP),
            P(TP),
            P(TP, FS),
        ),
        out_specs=P(REP_FS, TP),
        check_vma=False,
    )
```

```python
import jax
import jax.numpy as jnp
from jax import lax
from jax.experimental import pallas as pl
from jax.experimental.pallas import tpu as pltpu
from jax.sharding import Mesh
from jax.sharding import PartitionSpec as P


REP, ZLO, X, Y, CORE = "rep", "fs_0", "fs_1", "tp_0", "tp_1"
TP = (Y, CORE)
FS = (ZLO, X)
REP_FS = (REP, ZLO, X)
RING = 4
BF16 = jnp.bfloat16
F32 = jnp.float32
LANES = 128

epsilon = 1e-06


def shift(value, axes, size, by):
    return lax.ppermute(value, axes, [(i, (i + by) % size) for i in range(size)])


def shift_x(value, by):
    return shift(value, X, RING, by)


def shift_y(value, by):
    return shift(value, Y, RING, by)


def swap_core(value):
    return shift(value, CORE, 2, 1)


def shift_apart(value, axes, size, by):
    pairs = [(2 * i + c, 2 * ((i + by * (1 - 2 * c)) % size) + c) for i in range(size) for c in range(2)]
    return lax.ppermute(value, (*axes, CORE), pairs)


def gather_ring(value, axes, size):
    first = shift_apart(value, axes, size, 1)
    second = shift_apart(value, axes, size, -1)
    return [value, first, second, shift_apart(first, axes, size, 1)]


def gather_z(block):
    return gather_ring(block, (REP, ZLO), 2 * RING)


def order_before(core):
    return 0, 1 + 2 * core, RING - 1 - 2 * core, 2


def order_z(core):
    return 0, RING - 1 - 2 * core, 1 + 2 * core, 2


def trade(value, flip):
    pairs = [
        (2 * i + c, 2 * (2 * c + (i % 2 if not flip else 1 - i % 2)) + i // 2)
        for i in range(RING)
        for c in range(2)
    ]
    return lax.ppermute(value, (X, CORE), pairs)


def kernel_call(body, outs, flops=0, scratch=(), hbm_in=(), hbm_out=(), limit=16):
    def run(*args):
        def spec(at, where):
            return pl.BlockSpec(memory_space=pltpu.HBM if at in where else pltpu.VMEM)

        return pl.pallas_call(
            body,
            out_shape=[jax.ShapeDtypeStruct(*out) for out in outs],
            in_specs=[spec(i, hbm_in) for i in range(len(args))],
            out_specs=[spec(i, hbm_out) for i in range(len(outs))],
            scratch_shapes=list(scratch),
            cost_estimate=pl.CostEstimate(flops=flops, bytes_accessed=0, transcendentals=0),
            compiler_params=pltpu.CompilerParams(vmem_limit_bytes=limit << 20),
        )(*args)

    return run


def place():
    return tuple(lax.axis_index(axis) for axis in (ZLO, X, Y, CORE))


def aligned(start, size):
    return pl.ds(pl.multiple_of(start, size), size)


def dot(left, right):
    return jnp.dot(left, right, preferred_element_type=F32)


def dot_t(left, right):
    return lax.dot_general(left, right, (((1,), (1,)), ((), ())), preferred_element_type=F32)


def two_parts(values):
    high = values.astype(BF16)
    return high, (values - high.astype(F32)).astype(BF16)


def gelu_exact(values):
    return 0.5 * values * (1.0 + lax.erf(values * (0.5**0.5)))


def rms(values, gain):
    return values * lax.rsqrt(jnp.mean(values * values, axis=-1, keepdims=True) + epsilon) * gain


def body(
    tokens,
    mixer_gain,
    gate_proj,
    value_proj,
    value_gain,
    spatial_mix,
    spatial_bias,
    head_gain,
    merge_proj,
    ffn_gain,
    gate_up,
    value_up,
    gate_kernel,
    value_kernel,
    gate_offset,
    value_offset,
    down_proj,
):
    length, features = tokens.shape
    heads, rows, _ = spatial_mix.shape
    part, width = gate_proj.shape
    inner = gate_up.shape[1]
    full = mixer_gain.shape[0]
    half = length // 2
    span = RING * part
    all_rows = RING * length
    own_rows = 2 * length
    padded = -(-inner // LANES) * LANES
    extra_rows = heads * rows
    pack_rows = 3 * part + extra_rows

    def turn(x, xs):
        return (x - xs) % RING

    gains = jnp.stack([mixer_gain, ffn_gain]).reshape(-1, part)

    def move(*moves):
        *pairs, sems = moves
        copies = [pltpu.make_async_copy(a, b, sems.at[i]) for i, (a, b) in enumerate(pairs)]
        for copy in copies:
            copy.start()
        for copy in copies:
            copy.wait()

    def entry_body(tokens, gate, value, merge, spatial, near, far, pack, sems):
        x = place()[1]
        move(
            (tokens.at[:, aligned(part * (x % 2), part)], near),
            (tokens.at[:, aligned(part * (1 - x % 2), part)], far),
            (gate, pack.at[0:part]),
            (value, pack.at[part : 2 * part]),
            (merge, pack.at[2 * part : 3 * part]),
            (spatial, pack.at[3 * part : pack_rows, 0:LANES]),
            sems,
        )

    piece = ((length, part), BF16)
    near, far, pack = kernel_call(
        entry_body,
        [piece, piece, ((pack_rows, part), BF16)],
        scratch=[pltpu.SemaphoreType.DMA((6,))],
        hbm_in=range(5),
        limit=62,
    )(tokens, gate_proj, value_proj, merge_proj, spatial_mix.reshape(extra_rows, length))
    near, far = trade(near, False), trade(far, True)

    packs = gather_z(pack)

    def join_body(gate, value, out, both, sems):
        move((gate, both.at[0:inner]), (value, both.at[inner : 2 * inner]), sems)
        move((both, out), sems)

    (up,) = kernel_call(
        join_body,
        [((2 * inner, part), BF16)],
        scratch=[pltpu.VMEM((2 * inner, part), BF16), pltpu.SemaphoreType.DMA((2,))],
        hbm_in=range(2),
        hbm_out=range(1),
        limit=62,
    )(gate_up.T, value_up.T)
    ups = gather_z(up)
    downs = gather_z(down_proj)

    def column_body(near, far, out):
        out[0:length] = near[...]
        out[length:] = far[...]

    (column,) = kernel_call(column_body, [((own_rows, part), BF16)])(near, far)
    columns = [column] + [shift_y(column, k) for k in range(1, RING)]

    def stack_body(*refs):
        for k in range(RING):
            refs[RING][k] = refs[k][...]

    (own,) = kernel_call(stack_body, [((RING, own_rows, part), BF16)])(*columns)
    other = swap_core(own)

    def project_body(*refs):
        own, other, weights = refs[0], refs[1], refs[2:6]
        gain, raw, pays = refs[6], refs[7], refs[8:12]
        z, x, y, core = place()
        for side, blocks in ((core, own), (1 - core, other)):
            for k in range(RING):
                j = (y - z - k) % RING
                for i in range(2):
                    xs = 2 * side + (x + i) % 2
                    raw[j, aligned(length * turn(x, xs), length), :] = blocks[
                        k, i * length : (i + 1) * length
                    ]
        squares = jnp.zeros((all_rows, 1), F32)
        gate = jnp.zeros((all_rows, width), F32)
        value = jnp.zeros((all_rows, width), F32)
        for j, weight in zip(order_z(core), weights):
            block = raw[j].astype(F32)
            squares = squares + jnp.sum(block * block, axis=1, keepdims=True)
            at = RING * ((z + j) % RING) + x
            scaled = (block * gain[pl.ds(at, 1), :]).astype(BF16)
            gate = gate + dot(scaled, weight[0:part])
            value = value + dot(scaled, weight[part : 2 * part])
        for t in range(RING):
            at = slice(t * length, (t + 1) * length)
            pays[t][:, :width] = gate[at].astype(BF16)
            pays[t][:, width : 2 * width] = value[at].astype(BF16)
            for j in range(RING):
                pays[t][extra_rows * j : extra_rows * (j + 1), 2 * width :] = weights[j][
                    3 * part :, :LANES
                ]
            row = jnp.broadcast_to(squares[at], (length, length)).T
            high, low = two_parts(row)
            base = RING * extra_rows
            pays[t][base : base + 16, 2 * width :] = high[:16]
            pays[t][base + 16 : base + 32, 2 * width :] = low[:16]
            pays[t][base + 32 :, 2 * width :] = jnp.zeros((length - base - 32, LANES), BF16)

    pay_shape = ((length, 2 * width + LANES), BF16)
    raw, *pays = kernel_call(
        project_body,
        [((RING, all_rows, part), BF16)] + [pay_shape] * RING,
        flops=2 * all_rows * span * 2 * width,
    )(own, other, *packs, gains)
    pays = [pays[0]] + [shift_x(pays[t], -t) for t in range(1, RING)]

    def mix_body(*refs):
        pays, (value_gain, bias, head_gain), out, matrix = refs[0:4], refs[4:7], refs[7], refs[8]
        z, x, _, core = place()
        base = RING * extra_rows
        squares = jnp.zeros((1, length), F32)
        total = jnp.zeros((length, 2 * width), F32)
        for t in range(RING):
            total = total + pays[t][:, : 2 * width].astype(F32)
            squares = squares + pays[t][base : base + 16, 2 * width :].astype(F32)[0:1]
            squares = squares + pays[t][base + 16 : base + 32, 2 * width :].astype(F32)[0:1]
            for i, j in enumerate(order_z(core)):
                block = pays[t][extra_rows * i : extra_rows * (i + 1), 2 * width :].astype(F32)
                at = rows * (RING * ((z + j) % RING) + (x + t) % RING)
                for h in range(heads):
                    matrix[h, aligned(at, rows), :] = block[h * rows : (h + 1) * rows]
        scale = jnp.broadcast_to(lax.rsqrt(squares / full + epsilon), (length, length)).T
        for h in range(heads):
            at = slice(h * length, (h + 1) * length)
            gated = gelu_exact((total[:, at] * scale).astype(BF16).astype(F32))
            at = slice(width + h * length, width + (h + 1) * length)
            spread = gelu_exact((total[:, at] * scale).astype(BF16).astype(F32))
            spread = rms(spread, value_gain[h : h + 1, :]).astype(BF16)
            mixed = dot(matrix[h].astype(BF16), spread)
            mixed = mixed + jnp.broadcast_to(bias[h : h + 1, :], (length, length)).T
            joined = rms(gated * mixed, head_gain[h : h + 1, :])
            out[:, h * length : (h + 1) * length] = joined.astype(BF16)

    (merged,) = kernel_call(
        mix_body,
        [((length, width), BF16)],
        flops=1 << 22,
        scratch=[pltpu.VMEM((heads, length, length), F32)],
    )(*pays, value_gain, spatial_bias, head_gain)
    merges = [merged] + [shift_x(merged, k) for k in range(1, RING)]

    def side_of(blocks, order, scratch, x, side):
        for t, block in zip(order, blocks):
            scratch[t] = block[...]
        return jnp.concatenate([scratch[turn(x, 2 * side + i)] for i in range(2)], 0)

    def merge_other_body(*refs):
        merges, weights, out, blocks = refs[0:4], refs[4:8], refs[8], refs[9]
        _, x, _, core = place()
        left = side_of(merges, range(RING), blocks, x, 1 - core)
        for j, weight in zip(order_z(core), weights):
            out[:, aligned(j * part, part)] = dot(left, weight[2 * part : 3 * part]).astype(BF16)

    merge_flops = 2 * own_rows * width * span
    merge_scratch = pltpu.VMEM((RING, length, width), BF16)
    (other,) = kernel_call(
        merge_other_body, [((own_rows, span), BF16)], flops=merge_flops, scratch=[merge_scratch]
    )(*merges, *packs)
    received = swap_core(other)

    def merge_own_body(*refs):
        merges, weights, received, raw = refs[0:4], refs[4:8], refs[8], refs[9]
        keep, sends, total, blocks = refs[10], refs[11:14], refs[14], refs[15]
        _, x, y, core = place()
        left = side_of(merges, range(RING), blocks, x, core)
        for j, weight in zip(order_z(core), weights):
            at = aligned(j * part, part)
            total[:, at] = dot(left, weight[2 * part : 3 * part]) + received[:, at].astype(F32)
        mine = aligned(half * y, half)
        tokens = aligned(length * turn(x, 2 * core + y // 2) + half * (y % 2), half)
        for j in range(RING):
            at = slice(j * part, (j + 1) * part)
            keep[:, at] = total[mine, at] + raw[j, tokens, :].astype(F32)
        for k in range(1, RING):
            sends[k - 1][...] = total[aligned(half * ((y + k) % RING), half), :].astype(BF16)

    keep, *sends = kernel_call(
        merge_own_body,
        [((half, span), F32)] + [((half, span), BF16)] * 3,
        flops=merge_flops,
        scratch=[pltpu.VMEM((own_rows, span), F32), merge_scratch],
    )(*merges, *packs, received, raw)
    sums = [shift_y(sends[k - 1], k) for k in range(1, RING)]

    def hidden_body(keep, first, second, third, out):
        total = keep[...] + first[...].astype(F32) + second[...].astype(F32)
        out[...] = (total + third[...].astype(F32)).astype(BF16)

    (hidden,) = kernel_call(hidden_body, [((half, span), BF16)])(keep, *sums)

    mine = [hidden] + [shift_y(hidden, k) for k in range(1, RING)]
    (mine,) = kernel_call(stack_body, [((RING, half, span), BF16)])(*mine)
    theirs = swap_core(mine)

    spare = padded - inner

    def over_tiles(run):
        def step(n, carry):
            start = pl.multiple_of(n * part, part)
            run(pl.ds(start, part), pl.ds(pl.multiple_of(inner + start, 32), part))
            return carry

        lax.fori_loop(0, inner // part, step, 0)
        rest = inner // part * part
        run(slice(rest, inner), slice(inner + rest, 2 * inner))

    def up_dot(left, weights, last, at):
        split = (RING - 1) * part
        return dot_t(left[:, :split], weights[at]) + dot_t(left[:, split:], last[at])

    def load_body(gate, value, first, second, out, sems):
        move(
            (gate, out.at[0:inner, 0:part]),
            (value, out.at[inner : 2 * inner, 0:part]),
            (first, out.at[:, part : 2 * part]),
            (second, out.at[:, 2 * part : 3 * part]),
            sems,
        )

    load_sems = pltpu.SemaphoreType.DMA((RING,))
    (weights,) = kernel_call(
        load_body, [((2 * inner, 3 * part), BF16)], scratch=[load_sems], hbm_in=range(4)
    )(gate_up.T, value_up.T, ups[1], ups[2])

    def up_far_body(*refs):
        mine, theirs, gain, weights, last_in = refs[0:5]
        gate_out, value_out, scaled, parts, last, sem = refs[5:11]
        z, x, y, core = place()
        copy = pltpu.make_async_copy(last_in, last, sem.at[0])
        copy.start()
        lane = lax.broadcasted_iota(jnp.int32, (half, LANES), 1)
        for side, block in ((core, mine), (1 - core, theirs)):
            for k in range(RING):
                ys = (y - k) % RING
                at = aligned(half * (ys % 2), half)
                t = turn(x, 2 * side + ys // 2)
                slot = jnp.where(t == 0, 3, jnp.where(t == 2, 0, (t + 1) // 2))
                squares = jnp.zeros((half, 1), F32)
                for i, j in enumerate(order_z(core)):
                    piece = block[k, :, aligned(j * part, part)].astype(F32)
                    squares = squares + jnp.sum(piece * piece, axis=1, keepdims=True)
                    row = gain[pl.ds(RING * (RING + (z + j) % RING) + x, 1), :]
                    scaled[slot, at, i * part : (i + 1) * part] = (piece * row).astype(BF16)
                high, low = two_parts(squares)
                high = jnp.broadcast_to(high.astype(F32), (half, LANES))
                low = jnp.broadcast_to(low.astype(F32), (half, LANES))
                parts[slot, at] = jnp.where(lane == 0, high, jnp.where(lane == 1, low, 0.0))
        copy.wait()

        def run(at, value_at):
            gate_out[:, at] = up_dot(scaled[0], weights, last, at).astype(BF16)
            value_out[:, at] = up_dot(scaled[0], weights, last, value_at).astype(BF16)

        over_tiles(run)
        gate_out[:, inner:] = parts[0, :, :spare].astype(BF16)

    up_flops = 2 * length * span * inner
    gate_shape, value_shape = (length, padded), (length, inner)
    gate_two, value_two, scaled, parts, last = kernel_call(
        up_far_body,
        [
            (gate_shape, BF16),
            (value_shape, BF16),
            ((RING, length, span), BF16),
            ((RING, length, LANES), F32),
            ((2 * inner, part), BF16),
        ],
        flops=2 * up_flops,
        scratch=[pltpu.SemaphoreType.DMA((1,))],
        hbm_in=range(4, 5),
        limit=24,
    )(mine, theirs, gains, weights, ups[3])
    gate_two = shift_x(gate_two, 1)
    value_two = shift_x(value_two, -1)

    def up_near_body(scaled, parts, weights, last, *outs):
        gate_out, value_out, gate_add, value_add, gate_own, value_own = outs
        left = scaled[1:RING].reshape((RING - 1) * length, span)

        def run(at, value_at):
            piece = up_dot(left, weights, last, at)
            gate_out[:, at] = piece[:length].astype(BF16)
            gate_add[:, at] = piece[length : 2 * length]
            gate_own[:, at] = piece[2 * length :]
            piece = up_dot(left, weights, last, value_at)
            value_add[:, at] = piece[:length]
            value_out[:, at] = piece[length : 2 * length].astype(BF16)
            value_own[:, at] = piece[2 * length :]

        over_tiles(run)
        gate_out[:, inner:] = parts[1, :, :spare].astype(BF16)
        gate_add[:, inner:] = parts[2, :, :spare]
        gate_own[:, inner:] = parts[3, :, :spare]

    gate_near, value_near, gate_add, value_add, gate_own, value_own = kernel_call(
        up_near_body,
        [(gate_shape, BF16), (value_shape, BF16)] + [(gate_shape, F32), (value_shape, F32)] * 2,
        flops=6 * up_flops,
        limit=24,
    )(scaled, parts, weights, last)
    gate_near = shift_x(gate_near, -1)
    value_near = shift_x(value_near, 1)

    def up_join_body(gate_two, value_two, gate_add, value_add, gate_out, value_out):
        def step(n, carry):
            at = aligned(n * 16, 16)
            gate_out[at] = (gate_two[at].astype(F32) + gate_add[at]).astype(BF16)
            value_out[at] = (value_two[at].astype(F32) + value_add[at]).astype(BF16)
            return carry

        lax.fori_loop(0, length // 16, step, 0)
        total = gate_two[:, inner:].astype(F32) + gate_add[:, inner:]
        high, low = two_parts(total[:, 0:1] + total[:, 1:2])
        gate_out[:, inner : inner + 1] = high
        gate_out[:, inner + 1 : inner + 2] = low

    gate_join, value_join = kernel_call(
        up_join_body, [(gate_shape, BF16), (value_shape, BF16)]
    )(gate_two, value_two, gate_add, value_add)
    gate_join = shift_x(gate_join, 1)
    value_join = shift_x(value_join, -1)

    def active_body(
        gate_own, gate_near, gate_join, value_own, value_near, value_join,
        gate_kernel, value_kernel, gate_offset, value_offset, out,
    ):
        gates, values = (gate_own, gate_near, gate_join), (value_own, value_near, value_join)
        squares = jnp.zeros((length, 1), F32)
        for ref in gates:
            squares = squares + ref[:, inner : inner + 1].astype(F32)
            squares = squares + ref[:, inner + 1 : inner + 2].astype(F32)
        scale = lax.rsqrt(squares / full + epsilon)

        def run(at, size):
            position = lax.broadcasted_iota(jnp.int32, (length, size), 0)

            def convolve(refs, kernel, offset):
                total = refs[0][:, at] + refs[1][:, at].astype(F32) + refs[2][:, at].astype(F32)
                pre = (total * scale).astype(BF16).astype(F32)
                before = jnp.where(position == 0, 0.0, pltpu.roll(pre, 1, 0))
                after = jnp.where(position == length - 1, 0.0, pltpu.roll(pre, length - 1, 0))
                taps = before * kernel[0:1, at] + pre * kernel[1:2, at] + after * kernel[2:3, at]
                return offset[:, at] + taps

            gate = convolve(gates, gate_kernel, gate_offset)
            value = convolve(values, value_kernel, value_offset)
            out[:, at] = (gelu_exact(gate) * value).astype(BF16)

        def step(n, carry):
            run(aligned(n * LANES, LANES), LANES)
            return carry

        lax.fori_loop(0, inner // LANES, step, 0)
        rest = inner // LANES * LANES
        run(slice(rest, inner), inner - rest)

    (active,) = kernel_call(active_body, [((length, inner), BF16)], flops=1 << 24)(
        gate_own, gate_near, gate_join, value_own, value_near, value_join,
        gate_kernel, value_kernel, gate_offset[None], value_offset[None],
    )
    actives = gather_ring(active, (X,), RING)

    def down_load_body(*refs):
        order = order_z(place()[3])
        move(*((refs[i], refs[RING].at[j]) for i, j in enumerate(order)), refs[RING + 1])

    (weights,) = kernel_call(
        down_load_body, [((RING, inner, part), BF16)], scratch=[load_sems], hbm_in=range(4)
    )(*downs)


    def down_body(side_is_own):
        def run(*refs):
            actives, weights, out, blocks, left = refs[0:4], refs[4], refs[5], refs[6], refs[7]
            _, x, _, core = place()
            side = core if side_is_own else 1 - core
            left[...] = side_of(actives, order_before(core), blocks, x, side)

            def step(j, carry):
                out[j] = dot(left[...], weights[j]).astype(out.dtype)
                return carry

            lax.fori_loop(0, RING, step, 0, unroll=2)

        return kernel_call(
            run,
            [((RING, own_rows, part), F32 if side_is_own else BF16)],
            flops=2 * own_rows * inner * span,
            scratch=[pltpu.VMEM((RING, length, inner), BF16), pltpu.VMEM((own_rows, inner), BF16)],
        )

    (other,) = down_body(False)(*actives, weights)
    received = swap_core(other)
    (own,) = down_body(True)(*actives, weights)

    def down_add_body(*refs):
        own, received, mine, keep, sends = refs[0], refs[1], refs[2], refs[3], refs[4:7]
        z, _, y, _ = place()
        at = (y - z) % RING
        for k in range(1, RING):
            j = (at + k) % RING
            sends[k - 1][...] = (own[j] + received[j].astype(F32)).astype(BF16)
        keep[...] = own[at] + received[at].astype(F32)
        for k in range(RING):
            place_rows = aligned(half * ((y - k) % RING), half)
            for j in range(RING):

                @pl.when(at == j)
                def _():
                    piece = mine[k, :, j * part : (j + 1) * part].astype(F32)
                    keep[place_rows, :] = keep[place_rows, :] + piece

    block = (own_rows, part)
    keep, *sends = kernel_call(
        down_add_body, [(block, F32)] + [(block, BF16)] * 3, flops=1 << 20
    )(own, received, mine)
    sums = [shift_y(sends[k - 1], k) for k in range(1, RING)]

    def result_body(keep, first, second, third, near, far, total):
        x = place()[1]
        added = keep[...] + first[...].astype(F32) + second[...].astype(F32)
        total[...] = added + third[...].astype(F32)
        near[...] = total[aligned(length * (x % 2), length), :].astype(BF16)
        far[...] = total[aligned(length * (1 - x % 2), length), :].astype(BF16)

    near, far = kernel_call(
        result_body, [piece, piece], scratch=[pltpu.VMEM(block, F32)]
    )(keep, *sums)

    near, far = trade(near, False), trade(far, True)

    def exit_body(near, far, out, sems):
        x = place()[1]
        move(
            (near, out.at[:, aligned(part * (x % 2), part)]),
            (far, out.at[:, aligned(part * (1 - x % 2), part)]),
            sems,
        )

    (out,) = kernel_call(
        exit_body,
        [((length, features), BF16)],
        scratch=[pltpu.SemaphoreType.DMA((2,))],
        hbm_in=range(2),
        hbm_out=range(1),
    )(near, far)
    return out


def solution(mesh):
    finer = Mesh(
        mesh.devices.reshape(mesh.shape["rep"], RING, RING, RING, 2), (REP, ZLO, X, Y, CORE)
    )

    return jax.shard_map(
        body,
        mesh=finer,
        in_specs=(
            P(REP_FS, TP),
            P(),
            P(FS, TP),
            P(FS, TP),
            P(TP, None),
            P(TP, FS, None),
            P(TP, None),
            P(TP, None),
            P(TP, FS),
            P(),
            P(FS, TP),
            P(FS, TP),
            P(None, TP),
            P(None, TP),
            P(TP),
            P(TP),
            P(TP, FS),
        ),
        out_specs=P(REP_FS, TP),
        check_vma=False,
    )
```

```python
import jax
import jax.numpy as jnp
from jax import lax
from jax.experimental import pallas as pl
from jax.experimental.pallas import tpu as pltpu
from jax.sharding import Mesh
from jax.sharding import PartitionSpec as P


REP, ZLO, X, Y, CORE = "rep", "fs_0", "fs_1", "tp_0", "tp_1"
TP = (Y, CORE)
FS = (ZLO, X)
REP_FS = (REP, ZLO, X)
RING = 4
BF16 = jnp.bfloat16
F32 = jnp.float32
LANES = 128

epsilon = 1e-06


def shift(value, axes, size, by):
    return lax.ppermute(value, axes, [(i, (i + by) % size) for i in range(size)])


def shift_x(value, by):
    return shift(value, X, RING, by)


def shift_y(value, by):
    return shift(value, Y, RING, by)


def swap_core(value):
    return shift(value, CORE, 2, 1)


def shift_apart(value, axes, size, by):
    pairs = [(2 * i + c, 2 * ((i + by * (1 - 2 * c)) % size) + c) for i in range(size) for c in range(2)]
    return lax.ppermute(value, (*axes, CORE), pairs)


def gather_ring(value, axes, size):
    first = shift_apart(value, axes, size, 1)
    second = shift_apart(value, axes, size, -1)
    return [value, first, second, shift_apart(first, axes, size, 1)]


def gather_z(block):
    return gather_ring(block, (REP, ZLO), 2 * RING)


def order_before(core):
    return 0, 1 + 2 * core, RING - 1 - 2 * core, 2


def order_z(core):
    return 0, RING - 1 - 2 * core, 1 + 2 * core, 2


def trade(value, flip):
    pairs = [
        (2 * i + c, 2 * (2 * c + (i % 2 if not flip else 1 - i % 2)) + i // 2)
        for i in range(RING)
        for c in range(2)
    ]
    return lax.ppermute(value, (X, CORE), pairs)


def kernel_call(body, outs, flops=0, scratch=(), hbm_in=(), hbm_out=(), limit=16):
    def run(*args):
        def spec(at, where):
            return pl.BlockSpec(memory_space=pltpu.HBM if at in where else pltpu.VMEM)

        return pl.pallas_call(
            body,
            out_shape=[jax.ShapeDtypeStruct(*out) for out in outs],
            in_specs=[spec(i, hbm_in) for i in range(len(args))],
            out_specs=[spec(i, hbm_out) for i in range(len(outs))],
            scratch_shapes=list(scratch),
            cost_estimate=pl.CostEstimate(flops=flops, bytes_accessed=0, transcendentals=0),
            compiler_params=pltpu.CompilerParams(vmem_limit_bytes=limit << 20),
        )(*args)

    return run


def place():
    return tuple(lax.axis_index(axis) for axis in (ZLO, X, Y, CORE))


def aligned(start, size):
    return pl.ds(pl.multiple_of(start, size), size)


def dot(left, right):
    return jnp.dot(left, right, preferred_element_type=F32)


def dot_t(left, right):
    return lax.dot_general(left, right, (((1,), (1,)), ((), ())), preferred_element_type=F32)


def two_parts(values):
    high = values.astype(BF16)
    return high, (values - high.astype(F32)).astype(BF16)


def gelu_exact(values):
    return 0.5 * values * (1.0 + lax.erf(values * (0.5**0.5)))


def rms(values, gain):
    return values * lax.rsqrt(jnp.mean(values * values, axis=-1, keepdims=True) + epsilon) * gain


def body(
    tokens,
    mixer_gain,
    gate_proj,
    value_proj,
    value_gain,
    spatial_mix,
    spatial_bias,
    head_gain,
    merge_proj,
    ffn_gain,
    gate_up,
    value_up,
    gate_kernel,
    value_kernel,
    gate_offset,
    value_offset,
    down_proj,
):
    length, features = tokens.shape
    heads, rows, _ = spatial_mix.shape
    part, width = gate_proj.shape
    inner = gate_up.shape[1]
    full = mixer_gain.shape[0]
    half = length // 2
    span = RING * part
    all_rows = RING * length
    own_rows = 2 * length
    padded = -(-inner // LANES) * LANES
    extra_rows = heads * rows
    pack_rows = 3 * part + extra_rows

    def turn(x, xs):
        return (x - xs) % RING

    gains = jnp.stack([mixer_gain, ffn_gain]).reshape(-1, part)

    def move(*moves):
        *pairs, sems = moves
        copies = [pltpu.make_async_copy(a, b, sems.at[i]) for i, (a, b) in enumerate(pairs)]
        for copy in copies:
            copy.start()
        for copy in copies:
            copy.wait()

    def entry_body(tokens, gate, value, merge, spatial, near, far, pack, sems):
        x = place()[1]
        move(
            (tokens.at[:, aligned(part * (x % 2), part)], near),
            (tokens.at[:, aligned(part * (1 - x % 2), part)], far),
            (gate, pack.at[0:part]),
            (value, pack.at[part : 2 * part]),
            (merge, pack.at[2 * part : 3 * part]),
            (spatial, pack.at[3 * part : pack_rows, 0:LANES]),
            sems,
        )

    piece = ((length, part), BF16)
    near, far, pack = kernel_call(
        entry_body,
        [piece, piece, ((pack_rows, part), BF16)],
        scratch=[pltpu.SemaphoreType.DMA((6,))],
        hbm_in=range(5),
        limit=62,
    )(tokens, gate_proj, value_proj, merge_proj, spatial_mix.reshape(extra_rows, length))
    near, far = trade(near, False), trade(far, True)

    packs = gather_z(pack)

    def join_body(gate, value, out, both, sems):
        move((gate, both.at[0:inner]), (value, both.at[inner : 2 * inner]), sems)
        move((both, out), sems)

    (up,) = kernel_call(
        join_body,
        [((2 * inner, part), BF16)],
        scratch=[pltpu.VMEM((2 * inner, part), BF16), pltpu.SemaphoreType.DMA((2,))],
        hbm_in=range(2),
        hbm_out=range(1),
        limit=61,
    )(gate_up.T, value_up.T)
    ups = gather_z(up)
    downs = gather_z(down_proj)

    def column_body(near, far, out):
        out[0:length] = near[...]
        out[length:] = far[...]

    (column,) = kernel_call(column_body, [((own_rows, part), BF16)])(near, far)
    columns = [column] + [shift_y(column, k) for k in range(1, RING)]

    def stack_body(*refs):
        for k in range(RING):
            refs[RING][k] = refs[k][...]

    (own,) = kernel_call(stack_body, [((RING, own_rows, part), BF16)])(*columns)
    other = swap_core(own)

    def project_body(*refs):
        own, other, weights = refs[0], refs[1], refs[2:6]
        gain, raw, pays = refs[6], refs[7], refs[8:12]
        z, x, y, core = place()
        for side, blocks in ((core, own), (1 - core, other)):
            for k in range(RING):
                j = (y - z - k) % RING
                for i in range(2):
                    xs = 2 * side + (x + i) % 2
                    raw[j, aligned(length * turn(x, xs), length), :] = blocks[
                        k, i * length : (i + 1) * length
                    ]
        squares = jnp.zeros((all_rows, 1), F32)
        gate = jnp.zeros((all_rows, width), F32)
        value = jnp.zeros((all_rows, width), F32)
        for j, weight in zip(order_z(core), weights):
            block = raw[j].astype(F32)
            squares = squares + jnp.sum(block * block, axis=1, keepdims=True)
            at = RING * ((z + j) % RING) + x
            scaled = (block * gain[pl.ds(at, 1), :]).astype(BF16)
            gate = gate + dot(scaled, weight[0:part])
            value = value + dot(scaled, weight[part : 2 * part])
        for t in range(RING):
            at = slice(t * length, (t + 1) * length)
            pays[t][:, :width] = gate[at].astype(BF16)
            pays[t][:, width : 2 * width] = value[at].astype(BF16)
            for j in range(RING):
                pays[t][extra_rows * j : extra_rows * (j + 1), 2 * width :] = weights[j][
                    3 * part :, :LANES
                ]
            row = jnp.broadcast_to(squares[at], (length, length)).T
            high, low = two_parts(row)
            base = RING * extra_rows
            pays[t][base : base + 16, 2 * width :] = high[:16]
            pays[t][base + 16 : base + 32, 2 * width :] = low[:16]
            pays[t][base + 32 :, 2 * width :] = jnp.zeros((length - base - 32, LANES), BF16)

    pay_shape = ((length, 2 * width + LANES), BF16)
    raw, *pays = kernel_call(
        project_body,
        [((RING, all_rows, part), BF16)] + [pay_shape] * RING,
        flops=2 * all_rows * span * 2 * width,
    )(own, other, *packs, gains)
    pays = [pays[0]] + [shift_x(pays[t], -t) for t in range(1, RING)]

    def mix_body(*refs):
        pays, (value_gain, bias, head_gain), out, matrix = refs[0:4], refs[4:7], refs[7], refs[8]
        z, x, _, core = place()
        base = RING * extra_rows
        squares = jnp.zeros((1, length), F32)
        total = jnp.zeros((length, 2 * width), F32)
        for t in range(RING):
            total = total + pays[t][:, : 2 * width].astype(F32)
            squares = squares + pays[t][base : base + 16, 2 * width :].astype(F32)[0:1]
            squares = squares + pays[t][base + 16 : base + 32, 2 * width :].astype(F32)[0:1]
            for i, j in enumerate(order_z(core)):
                block = pays[t][extra_rows * i : extra_rows * (i + 1), 2 * width :].astype(F32)
                at = rows * (RING * ((z + j) % RING) + (x + t) % RING)
                for h in range(heads):
                    matrix[h, aligned(at, rows), :] = block[h * rows : (h + 1) * rows]
        scale = jnp.broadcast_to(lax.rsqrt(squares / full + epsilon), (length, length)).T
        for h in range(heads):
            at = slice(h * length, (h + 1) * length)
            gated = gelu_exact((total[:, at] * scale).astype(BF16).astype(F32))
            at = slice(width + h * length, width + (h + 1) * length)
            spread = gelu_exact((total[:, at] * scale).astype(BF16).astype(F32))
            spread = rms(spread, value_gain[h : h + 1, :]).astype(BF16)
            mixed = dot(matrix[h].astype(BF16), spread)
            mixed = mixed + jnp.broadcast_to(bias[h : h + 1, :], (length, length)).T
            joined = rms(gated * mixed, head_gain[h : h + 1, :])
            out[:, h * length : (h + 1) * length] = joined.astype(BF16)

    (merged,) = kernel_call(
        mix_body,
        [((length, width), BF16)],
        flops=1 << 22,
        scratch=[pltpu.VMEM((heads, length, length), F32)],
    )(*pays, value_gain, spatial_bias, head_gain)
    merges = [merged] + [shift_x(merged, k) for k in range(1, RING)]

    def side_of(blocks, order, scratch, x, side):
        for t, block in zip(order, blocks):
            scratch[t] = block[...]
        return jnp.concatenate([scratch[turn(x, 2 * side + i)] for i in range(2)], 0)

    def merge_other_body(*refs):
        merges, weights, out, blocks = refs[0:4], refs[4:8], refs[8], refs[9]
        _, x, _, core = place()
        left = side_of(merges, range(RING), blocks, x, 1 - core)
        for j, weight in zip(order_z(core), weights):
            out[:, aligned(j * part, part)] = dot(left, weight[2 * part : 3 * part]).astype(BF16)

    merge_flops = 2 * own_rows * width * span
    merge_scratch = pltpu.VMEM((RING, length, width), BF16)
    (other,) = kernel_call(
        merge_other_body,
        [((own_rows, span), BF16)],
        flops=merge_flops,
        scratch=[merge_scratch],
    )(*merges, *packs)
    received = swap_core(other)

    def merge_own_body(*refs):
        merges, weights, received, raw = refs[0:4], refs[4:8], refs[8], refs[9]
        keep, sends, total, blocks = refs[10], refs[11:14], refs[14], refs[15]
        _, x, y, core = place()
        left = side_of(merges, range(RING), blocks, x, core)
        for j, weight in zip(order_z(core), weights):
            at = aligned(j * part, part)
            total[:, at] = dot(left, weight[2 * part : 3 * part]) + received[:, at].astype(F32)
        mine = aligned(half * y, half)
        tokens = aligned(length * turn(x, 2 * core + y // 2) + half * (y % 2), half)
        for j in range(RING):
            at = slice(j * part, (j + 1) * part)
            keep[:, at] = total[mine, at] + raw[j, tokens, :].astype(F32)
        for k in range(1, RING):
            sends[k - 1][...] = total[aligned(half * ((y + k) % RING), half), :].astype(BF16)

    keep, *sends = kernel_call(
        merge_own_body,
        [((half, span), F32)] + [((half, span), BF16)] * 3,
        flops=merge_flops,
        scratch=[pltpu.VMEM((own_rows, span), F32), merge_scratch],
    )(*merges, *packs, received, raw)
    sums = [shift_y(sends[k - 1], k) for k in range(1, RING)]

    def hidden_body(keep, first, second, third, out):
        total = keep[...] + first[...].astype(F32) + second[...].astype(F32)
        out[...] = (total + third[...].astype(F32)).astype(BF16)

    (hidden,) = kernel_call(hidden_body, [((half, span), BF16)])(keep, *sums)

    mine = [hidden] + [shift_y(hidden, k) for k in range(1, RING)]
    (mine,) = kernel_call(stack_body, [((RING, half, span), BF16)])(*mine)
    theirs = swap_core(mine)

    spare = padded - inner

    def over_tiles(run):
        def step(n, carry):
            start = pl.multiple_of(n * part, part)
            run(pl.ds(start, part), pl.ds(pl.multiple_of(inner + start, 32), part))
            return carry

        lax.fori_loop(0, inner // part, step, 0)
        rest = inner // part * part
        run(slice(rest, inner), slice(inner + rest, 2 * inner))

    def up_dot(left, weights, last, at):
        split = (RING - 1) * part
        return dot_t(left[:, :split], weights[at]) + dot_t(left[:, split:], last[at])

    def load_body(gate, value, first, second, out, sems):
        move(
            (gate, out.at[0:inner, 0:part]),
            (value, out.at[inner : 2 * inner, 0:part]),
            (first, out.at[:, part : 2 * part]),
            (second, out.at[:, 2 * part : 3 * part]),
            sems,
        )

    load_sems = pltpu.SemaphoreType.DMA((RING,))
    (weights,) = kernel_call(
        load_body,
        [((2 * inner, 3 * part), BF16)],
        scratch=[load_sems],
        hbm_in=range(4),
    )(gate_up.T, value_up.T, ups[1], ups[2])

    def up_far_body(*refs):
        mine, theirs, gain, weights, last_in = refs[0:5]
        gate_out, value_out, scaled, parts, last, sem = refs[5:11]
        z, x, y, core = place()
        copy = pltpu.make_async_copy(last_in, last, sem.at[0])
        copy.start()
        lane = lax.broadcasted_iota(jnp.int32, (half, LANES), 1)
        for side, block in ((core, mine), (1 - core, theirs)):
            for k in range(RING):
                ys = (y - k) % RING
                at = aligned(half * (ys % 2), half)
                t = turn(x, 2 * side + ys // 2)
                slot = jnp.where(t == 0, 3, jnp.where(t == 2, 0, (t + 1) // 2))
                squares = jnp.zeros((half, 1), F32)
                for i, j in enumerate(order_z(core)):
                    piece = block[k, :, aligned(j * part, part)].astype(F32)
                    squares = squares + jnp.sum(piece * piece, axis=1, keepdims=True)
                    row = gain[pl.ds(RING * (RING + (z + j) % RING) + x, 1), :]
                    scaled[slot, at, i * part : (i + 1) * part] = (piece * row).astype(BF16)
                high, low = two_parts(squares)
                high = jnp.broadcast_to(high.astype(F32), (half, LANES))
                low = jnp.broadcast_to(low.astype(F32), (half, LANES))
                parts[slot, at] = jnp.where(lane == 0, high, jnp.where(lane == 1, low, 0.0))
        copy.wait()

        def run(at, value_at):
            gate_out[:, at] = up_dot(scaled[0], weights, last, at).astype(BF16)
            value_out[:, at] = up_dot(scaled[0], weights, last, value_at).astype(BF16)

        over_tiles(run)
        gate_out[:, inner:] = parts[0, :, :spare].astype(BF16)

    up_flops = 2 * length * span * inner
    gate_shape, value_shape = (length, padded), (length, inner)
    gate_two, value_two, scaled, parts, last = kernel_call(
        up_far_body,
        [
            (gate_shape, BF16),
            (value_shape, BF16),
            ((RING, length, span), BF16),
            ((RING, length, LANES), F32),
            ((2 * inner, part), BF16),
        ],
        flops=2 * up_flops,
        scratch=[pltpu.SemaphoreType.DMA((1,))],
        hbm_in=range(4, 5),
        limit=24,
    )(mine, theirs, gains, weights, ups[3])
    gate_two = shift_x(gate_two, 1)
    value_two = shift_x(value_two, -1)

    def up_near_body(scaled, parts, weights, last, *outs):
        gate_out, value_out, gate_add, value_add, gate_own, value_own = outs
        left = scaled[1:RING].reshape((RING - 1) * length, span)

        def run(at, value_at):
            piece = up_dot(left, weights, last, at)
            gate_out[:, at] = piece[:length].astype(BF16)
            gate_add[:, at] = piece[length : 2 * length]
            gate_own[:, at] = piece[2 * length :]
            piece = up_dot(left, weights, last, value_at)
            value_add[:, at] = piece[:length]
            value_out[:, at] = piece[length : 2 * length].astype(BF16)
            value_own[:, at] = piece[2 * length :]

        over_tiles(run)
        gate_out[:, inner:] = parts[1, :, :spare].astype(BF16)
        gate_add[:, inner:] = parts[2, :, :spare]
        gate_own[:, inner:] = parts[3, :, :spare]

    gate_near, value_near, gate_add, value_add, gate_own, value_own = kernel_call(
        up_near_body,
        [(gate_shape, BF16), (value_shape, BF16)] + [(gate_shape, F32), (value_shape, F32)] * 2,
        flops=6 * up_flops,
        limit=24,
    )(scaled, parts, weights, last)
    gate_near = shift_x(gate_near, -1)
    value_near = shift_x(value_near, 1)

    def up_join_body(gate_two, value_two, gate_add, value_add, gate_out, value_out):
        def step(n, carry):
            at = aligned(n * 16, 16)
            gate_out[at] = (gate_two[at].astype(F32) + gate_add[at]).astype(BF16)
            value_out[at] = (value_two[at].astype(F32) + value_add[at]).astype(BF16)
            return carry

        lax.fori_loop(0, length // 16, step, 0)
        total = gate_two[:, inner:].astype(F32) + gate_add[:, inner:]
        high, low = two_parts(total[:, 0:1] + total[:, 1:2])
        gate_out[:, inner : inner + 1] = high
        gate_out[:, inner + 1 : inner + 2] = low

    gate_join, value_join = kernel_call(
        up_join_body, [(gate_shape, BF16), (value_shape, BF16)]
    )(gate_two, value_two, gate_add, value_add)
    gate_join = shift_x(gate_join, 1)
    value_join = shift_x(value_join, -1)

    def active_body(
        gate_own, gate_near, gate_join, value_own, value_near, value_join,
        gate_kernel, value_kernel, gate_offset, value_offset, out,
    ):
        gates, values = (gate_own, gate_near, gate_join), (value_own, value_near, value_join)
        squares = jnp.zeros((length, 1), F32)
        for ref in gates:
            squares = squares + ref[:, inner : inner + 1].astype(F32)
            squares = squares + ref[:, inner + 1 : inner + 2].astype(F32)
        scale = lax.rsqrt(squares / full + epsilon)

        def run(at, size):
            position = lax.broadcasted_iota(jnp.int32, (length, size), 0)

            def convolve(refs, kernel, offset):
                total = refs[0][:, at] + refs[1][:, at].astype(F32) + refs[2][:, at].astype(F32)
                pre = (total * scale).astype(BF16).astype(F32)
                before = jnp.where(position == 0, 0.0, pltpu.roll(pre, 1, 0))
                after = jnp.where(position == length - 1, 0.0, pltpu.roll(pre, length - 1, 0))
                taps = before * kernel[0:1, at] + pre * kernel[1:2, at] + after * kernel[2:3, at]
                return offset[:, at] + taps

            gate = convolve(gates, gate_kernel, gate_offset)
            value = convolve(values, value_kernel, value_offset)
            out[:, at] = (gelu_exact(gate) * value).astype(BF16)

        def step(n, carry):
            run(aligned(n * LANES, LANES), LANES)
            return carry

        lax.fori_loop(0, inner // LANES, step, 0)
        rest = inner // LANES * LANES
        run(slice(rest, inner), inner - rest)

    (active,) = kernel_call(active_body, [((length, inner), BF16)], flops=1 << 24)(
        gate_own, gate_near, gate_join, value_own, value_near, value_join,
        gate_kernel, value_kernel, gate_offset[None], value_offset[None],
    )
    actives = gather_ring(active, (X,), RING)

    def down_load_body(*refs):
        order = order_z(place()[3])
        move(*((refs[i], refs[RING].at[j]) for i, j in enumerate(order)), refs[RING + 1])

    (weights,) = kernel_call(
        down_load_body,
        [((RING, inner, part), BF16)],
        scratch=[load_sems],
        hbm_in=range(4),
    )(*downs)


    def down_body(side_is_own):
        def run(*refs):
            actives, weights, out, blocks, left = refs[0:4], refs[4], refs[5], refs[6], refs[7]
            _, x, _, core = place()
            side = core if side_is_own else 1 - core
            left[...] = side_of(actives, order_before(core), blocks, x, side)

            def step(j, carry):
                out[j] = dot(left[...], weights[j]).astype(out.dtype)
                return carry

            lax.fori_loop(0, RING, step, 0, unroll=2)

        return kernel_call(
            run,
            [((RING, own_rows, part), F32 if side_is_own else BF16)],
            flops=2 * own_rows * inner * span,
            scratch=[pltpu.VMEM((RING, length, inner), BF16), pltpu.VMEM((own_rows, inner), BF16)],
        )

    (other,) = down_body(False)(*actives, weights)
    received = swap_core(other)
    (own,) = down_body(True)(*actives, weights)

    def down_add_body(*refs):
        own, received, mine, keep, sends = refs[0], refs[1], refs[2], refs[3], refs[4:7]
        z, _, y, _ = place()
        at = (y - z) % RING
        for k in range(1, RING):
            j = (at + k) % RING
            sends[k - 1][...] = (own[j] + received[j].astype(F32)).astype(BF16)
        keep[...] = own[at] + received[at].astype(F32)
        for k in range(RING):
            place_rows = aligned(half * ((y - k) % RING), half)
            for j in range(RING):

                @pl.when(at == j)
                def _():
                    piece = mine[k, :, j * part : (j + 1) * part].astype(F32)
                    keep[place_rows, :] = keep[place_rows, :] + piece

    block = (own_rows, part)
    keep, *sends = kernel_call(
        down_add_body, [(block, F32)] + [(block, BF16)] * 3, flops=1 << 20
    )(own, received, mine)
    sums = [shift_y(sends[k - 1], k) for k in range(1, RING)]

    def result_body(keep, first, second, third, near, far, total):
        x = place()[1]
        added = keep[...] + first[...].astype(F32) + second[...].astype(F32)
        total[...] = added + third[...].astype(F32)
        near[...] = total[aligned(length * (x % 2), length), :].astype(BF16)
        far[...] = total[aligned(length * (1 - x % 2), length), :].astype(BF16)

    near, far = kernel_call(
        result_body, [piece, piece], scratch=[pltpu.VMEM(block, F32)]
    )(keep, *sums)

    near, far = trade(near, False), trade(far, True)

    def exit_body(near, far, out, sems):
        x = place()[1]
        move(
            (near, out.at[:, aligned(part * (x % 2), part)]),
            (far, out.at[:, aligned(part * (1 - x % 2), part)]),
            sems,
        )

    (out,) = kernel_call(
        exit_body,
        [((length, features), BF16)],
        scratch=[pltpu.SemaphoreType.DMA((2,))],
        hbm_in=range(2),
        hbm_out=range(1),
    )(near, far)
    return out


def solution(mesh):
    finer = Mesh(
        mesh.devices.reshape(mesh.shape["rep"], RING, RING, RING, 2), (REP, ZLO, X, Y, CORE)
    )

    return jax.shard_map(
        body,
        mesh=finer,
        in_specs=(
            P(REP_FS, TP),
            P(),
            P(FS, TP),
            P(FS, TP),
            P(TP, None),
            P(TP, FS, None),
            P(TP, None),
            P(TP, None),
            P(TP, FS),
            P(),
            P(FS, TP),
            P(FS, TP),
            P(None, TP),
            P(None, TP),
            P(TP),
            P(TP),
            P(TP, FS),
        ),
        out_specs=P(REP_FS, TP),
        check_vma=False,
    )
```

```python
import jax
import jax.numpy as jnp
from jax import lax
from jax.experimental import pallas as pl
from jax.experimental.pallas import tpu as pltpu
from jax.sharding import Mesh
from jax.sharding import PartitionSpec as P


REP, ZLO, X, Y, CORE = "rep", "fs_0", "fs_1", "tp_0", "tp_1"
TP = (Y, CORE)
FS = (ZLO, X)
REP_FS = (REP, ZLO, X)
RING = 4
BF16 = jnp.bfloat16
F32 = jnp.float32
LANES = 128

epsilon = 1e-06


def shift(value, axes, size, by):
    return lax.ppermute(value, axes, [(i, (i + by) % size) for i in range(size)])


def shift_x(value, by):
    return shift(value, X, RING, by)


def shift_y(value, by):
    return shift(value, Y, RING, by)


def swap_core(value):
    return shift(value, CORE, 2, 1)


def shift_apart(value, axes, size, by):
    pairs = [(2 * i + c, 2 * ((i + by * (1 - 2 * c)) % size) + c) for i in range(size) for c in range(2)]
    return lax.ppermute(value, (*axes, CORE), pairs)


def gather_ring(value, axes, size):
    first = shift_apart(value, axes, size, 1)
    second = shift_apart(value, axes, size, -1)
    return [value, first, second, shift_apart(first, axes, size, 1)]


def gather_z(block):
    return gather_ring(block, (REP, ZLO), 2 * RING)


def order_before(core):
    return 0, 1 + 2 * core, RING - 1 - 2 * core, 2


def order_z(core):
    return 0, RING - 1 - 2 * core, 1 + 2 * core, 2


def trade(value, flip):
    pairs = [
        (2 * i + c, 2 * (2 * c + (i % 2 if not flip else 1 - i % 2)) + i // 2)
        for i in range(RING)
        for c in range(2)
    ]
    return lax.ppermute(value, (X, CORE), pairs)


def kernel_call(body, outs, flops=0, scratch=(), hbm_in=(), hbm_out=(), limit=16):
    def run(*args):
        def spec(at, where):
            return pl.BlockSpec(memory_space=pltpu.HBM if at in where else pltpu.VMEM)

        return pl.pallas_call(
            body,
            out_shape=[jax.ShapeDtypeStruct(*out) for out in outs],
            in_specs=[spec(i, hbm_in) for i in range(len(args))],
            out_specs=[spec(i, hbm_out) for i in range(len(outs))],
            scratch_shapes=list(scratch),
            cost_estimate=pl.CostEstimate(flops=flops, bytes_accessed=0, transcendentals=0),
            compiler_params=pltpu.CompilerParams(vmem_limit_bytes=limit << 20),
        )(*args)

    return run


def place():
    return tuple(lax.axis_index(axis) for axis in (ZLO, X, Y, CORE))


def aligned(start, size):
    return pl.ds(pl.multiple_of(start, size), size)


def dot(left, right):
    return jnp.dot(left, right, preferred_element_type=F32)


def dot_t(left, right):
    return lax.dot_general(left, right, (((1,), (1,)), ((), ())), preferred_element_type=F32)


def two_parts(values):
    high = values.astype(BF16)
    return high, (values - high.astype(F32)).astype(BF16)


def gelu_exact(values):
    return 0.5 * values * (1.0 + lax.erf(values * (0.5**0.5)))


def rms(values, gain):
    return values * lax.rsqrt(jnp.mean(values * values, axis=-1, keepdims=True) + epsilon) * gain


def body(
    tokens,
    mixer_gain,
    gate_proj,
    value_proj,
    value_gain,
    spatial_mix,
    spatial_bias,
    head_gain,
    merge_proj,
    ffn_gain,
    gate_up,
    value_up,
    gate_kernel,
    value_kernel,
    gate_offset,
    value_offset,
    down_proj,
):
    length, features = tokens.shape
    heads, rows, _ = spatial_mix.shape
    part, width = gate_proj.shape
    inner = gate_up.shape[1]
    full = mixer_gain.shape[0]
    half = length // 2
    span = RING * part
    all_rows = RING * length
    own_rows = 2 * length
    padded = -(-inner // LANES) * LANES
    extra_rows = heads * rows
    pack_rows = 3 * part + extra_rows

    def turn(x, xs):
        return (x - xs) % RING

    gains = jnp.stack([mixer_gain, ffn_gain]).reshape(-1, part)

    def move(*moves):
        *pairs, sems = moves
        copies = [pltpu.make_async_copy(a, b, sems.at[i]) for i, (a, b) in enumerate(pairs)]
        for copy in copies:
            copy.start()
        for copy in copies:
            copy.wait()

    def entry_body(tokens, gate, value, merge, spatial, near, far, pack, sems):
        x = place()[1]
        move(
            (tokens.at[:, aligned(part * (x % 2), part)], near),
            (tokens.at[:, aligned(part * (1 - x % 2), part)], far),
            (gate, pack.at[0:part]),
            (value, pack.at[part : 2 * part]),
            (merge, pack.at[2 * part : 3 * part]),
            (spatial, pack.at[3 * part : pack_rows, 0:LANES]),
            sems,
        )

    piece = ((length, part), BF16)
    near, far, pack = kernel_call(
        entry_body,
        [piece, piece, ((pack_rows, part), BF16)],
        scratch=[pltpu.SemaphoreType.DMA((6,))],
        hbm_in=range(5),
        limit=62,
    )(tokens, gate_proj, value_proj, merge_proj, spatial_mix.reshape(extra_rows, length))
    near, far = trade(near, False), trade(far, True)

    packs = gather_z(pack)

    def join_body(gate, value, out, both, sems):
        move((gate, both.at[0:inner]), (value, both.at[inner : 2 * inner]), sems)
        move((both, out), sems)

    (up,) = kernel_call(
        join_body,
        [((2 * inner, part), BF16)],
        scratch=[pltpu.VMEM((2 * inner, part), BF16), pltpu.SemaphoreType.DMA((2,))],
        hbm_in=range(2),
        hbm_out=range(1),
        limit=61,
    )(gate_up.T, value_up.T)
    ups = gather_z(up)
    downs = gather_z(down_proj)

    def column_body(near, far, out):
        out[0:length] = near[...]
        out[length:] = far[...]

    (column,) = kernel_call(column_body, [((own_rows, part), BF16)])(near, far)
    columns = [column] + [shift_y(column, k) for k in range(1, RING)]

    def stack_body(*refs):
        for k in range(RING):
            refs[RING][k] = refs[k][...]

    (own,) = kernel_call(stack_body, [((RING, own_rows, part), BF16)])(*columns)
    other = swap_core(own)

    def project_body(*refs):
        own, other, weights = refs[0], refs[1], refs[2:6]
        gain, raw, pays = refs[6], refs[7], refs[8:12]
        z, x, y, core = place()
        for side, blocks in ((core, own), (1 - core, other)):
            for k in range(RING):
                j = (y - z - k) % RING
                for i in range(2):
                    xs = 2 * side + (x + i) % 2
                    raw[j, aligned(length * turn(x, xs), length), :] = blocks[
                        k, i * length : (i + 1) * length
                    ]
        squares = jnp.zeros((all_rows, 1), F32)
        gate = jnp.zeros((all_rows, width), F32)
        value = jnp.zeros((all_rows, width), F32)
        for j, weight in zip(order_z(core), weights):
            block = raw[j].astype(F32)
            squares = squares + jnp.sum(block * block, axis=1, keepdims=True)
            at = RING * ((z + j) % RING) + x
            scaled = (block * gain[pl.ds(at, 1), :]).astype(BF16)
            gate = gate + dot(scaled, weight[0:part])
            value = value + dot(scaled, weight[part : 2 * part])
        for t in range(RING):
            at = slice(t * length, (t + 1) * length)
            pays[t][:, :width] = gate[at].astype(BF16)
            pays[t][:, width : 2 * width] = value[at].astype(BF16)
            for j in range(RING):
                pays[t][extra_rows * j : extra_rows * (j + 1), 2 * width :] = weights[j][
                    3 * part :, :LANES
                ]
            row = jnp.broadcast_to(squares[at], (length, length)).T
            high, low = two_parts(row)
            base = RING * extra_rows
            pays[t][base : base + 16, 2 * width :] = high[:16]
            pays[t][base + 16 : base + 32, 2 * width :] = low[:16]
            pays[t][base + 32 :, 2 * width :] = jnp.zeros((length - base - 32, LANES), BF16)

    pay_shape = ((length, 2 * width + LANES), BF16)
    raw, *pays = kernel_call(
        project_body,
        [((RING, all_rows, part), BF16)] + [pay_shape] * RING,
        flops=2 * all_rows * span * 2 * width,
    )(own, other, *packs, gains)
    pays = [pays[0]] + [shift_x(pays[t], -t) for t in range(1, RING)]

    def mix_body(*refs):
        pays, (value_gain, bias, head_gain), out, matrix = refs[0:4], refs[4:7], refs[7], refs[8]
        z, x, _, core = place()
        base = RING * extra_rows
        squares = jnp.zeros((1, length), F32)
        total = jnp.zeros((length, 2 * width), F32)
        for t in range(RING):
            total = total + pays[t][:, : 2 * width].astype(F32)
            squares = squares + pays[t][base : base + 16, 2 * width :].astype(F32)[0:1]
            squares = squares + pays[t][base + 16 : base + 32, 2 * width :].astype(F32)[0:1]
            for i, j in enumerate(order_z(core)):
                block = pays[t][extra_rows * i : extra_rows * (i + 1), 2 * width :].astype(F32)
                at = rows * (RING * ((z + j) % RING) + (x + t) % RING)
                for h in range(heads):
                    matrix[h, aligned(at, rows), :] = block[h * rows : (h + 1) * rows]
        scale = jnp.broadcast_to(lax.rsqrt(squares / full + epsilon), (length, length)).T
        for h in range(heads):
            at = slice(h * length, (h + 1) * length)
            gated = gelu_exact((total[:, at] * scale).astype(BF16).astype(F32))
            at = slice(width + h * length, width + (h + 1) * length)
            spread = gelu_exact((total[:, at] * scale).astype(BF16).astype(F32))
            spread = rms(spread, value_gain[h : h + 1, :]).astype(BF16)
            mixed = dot(matrix[h].astype(BF16), spread)
            mixed = mixed + jnp.broadcast_to(bias[h : h + 1, :], (length, length)).T
            joined = rms(gated * mixed, head_gain[h : h + 1, :])
            out[:, h * length : (h + 1) * length] = joined.astype(BF16)

    (merged,) = kernel_call(
        mix_body,
        [((length, width), BF16)],
        flops=1 << 22,
        scratch=[pltpu.VMEM((heads, length, length), F32)],
    )(*pays, value_gain, spatial_bias, head_gain)
    merges = [merged] + [shift_x(merged, k) for k in range(1, RING)]

    def side_of(blocks, order, scratch, x, side):
        for t, block in zip(order, blocks):
            scratch[t] = block[...]
        return jnp.concatenate([scratch[turn(x, 2 * side + i)] for i in range(2)], 0)

    def merge_other_body(*refs):
        merges, weights, out, blocks = refs[0:4], refs[4:8], refs[8], refs[9]
        _, x, _, core = place()
        left = side_of(merges, range(RING), blocks, x, 1 - core)
        for j, weight in zip(order_z(core), weights):
            out[:, aligned(j * part, part)] = dot(left, weight[2 * part : 3 * part]).astype(BF16)

    merge_flops = 2 * own_rows * width * span
    merge_scratch = pltpu.VMEM((RING, length, width), BF16)
    (other,) = kernel_call(
        merge_other_body,
        [((own_rows, span), BF16)],
        flops=merge_flops,
        scratch=[merge_scratch],
    )(*merges, *packs)
    received = swap_core(other)

    def merge_own_body(*refs):
        merges, weights, received, raw = refs[0:4], refs[4:8], refs[8], refs[9]
        keep, sends, total, blocks = refs[10], refs[11:14], refs[14], refs[15]
        _, x, y, core = place()
        left = side_of(merges, range(RING), blocks, x, core)
        for j, weight in zip(order_z(core), weights):
            at = aligned(j * part, part)
            total[:, at] = dot(left, weight[2 * part : 3 * part]) + received[:, at].astype(F32)
        mine = aligned(half * y, half)
        tokens = aligned(length * turn(x, 2 * core + y // 2) + half * (y % 2), half)
        for j in range(RING):
            at = slice(j * part, (j + 1) * part)
            keep[:, at] = total[mine, at] + raw[j, tokens, :].astype(F32)
        for k in range(1, RING):
            sends[k - 1][...] = total[aligned(half * ((y + k) % RING), half), :].astype(BF16)

    keep, *sends = kernel_call(
        merge_own_body,
        [((half, span), F32)] + [((half, span), BF16)] * 3,
        flops=merge_flops,
        scratch=[pltpu.VMEM((own_rows, span), F32), merge_scratch],
    )(*merges, *packs, received, raw)
    sums = [shift_y(sends[k - 1], k) for k in range(1, RING)]

    def hidden_body(keep, first, second, third, out):
        total = keep[...] + first[...].astype(F32) + second[...].astype(F32)
        out[...] = (total + third[...].astype(F32)).astype(BF16)

    (hidden,) = kernel_call(hidden_body, [((half, span), BF16)])(keep, *sums)

    mine = [hidden] + [shift_y(hidden, k) for k in range(1, RING)]
    (mine,) = kernel_call(stack_body, [((RING, half, span), BF16)])(*mine)
    theirs = swap_core(mine)

    spare = padded - inner

    def over_tiles(run, unroll=1):
        def step(n, carry):
            start = pl.multiple_of(n * part, part)
            run(pl.ds(start, part), pl.ds(pl.multiple_of(inner + start, 32), part))
            return carry

        lax.fori_loop(0, inner // part, step, 0, unroll=unroll)
        rest = inner // part * part
        run(slice(rest, inner), slice(inner + rest, 2 * inner))

    def up_dot(left, weights, last, at):
        split = (RING - 1) * part
        return dot_t(left[:, :split], weights[at]) + dot_t(left[:, split:], last[at])

    def load_body(gate, value, first, second, out, sems):
        move(
            (gate, out.at[0:inner, 0:part]),
            (value, out.at[inner : 2 * inner, 0:part]),
            (first, out.at[:, part : 2 * part]),
            (second, out.at[:, 2 * part : 3 * part]),
            sems,
        )

    load_sems = pltpu.SemaphoreType.DMA((RING,))
    (weights,) = kernel_call(
        load_body,
        [((2 * inner, 3 * part), BF16)],
        scratch=[load_sems],
        hbm_in=range(4),
    )(gate_up.T, value_up.T, ups[1], ups[2])

    def up_far_body(*refs):
        mine, theirs, gain, weights, last_in = refs[0:5]
        gate_out, value_out, scaled, parts, last, sem = refs[5:11]
        z, x, y, core = place()
        copy = pltpu.make_async_copy(last_in, last, sem.at[0])
        copy.start()
        lane = lax.broadcasted_iota(jnp.int32, (half, LANES), 1)
        for side, block in ((core, mine), (1 - core, theirs)):
            for k in range(RING):
                ys = (y - k) % RING
                at = aligned(half * (ys % 2), half)
                t = turn(x, 2 * side + ys // 2)
                slot = jnp.where(t == 0, 3, jnp.where(t == 2, 0, (t + 1) // 2))
                squares = jnp.zeros((half, 1), F32)
                for i, j in enumerate(order_z(core)):
                    piece = block[k, :, aligned(j * part, part)].astype(F32)
                    squares = squares + jnp.sum(piece * piece, axis=1, keepdims=True)
                    row = gain[pl.ds(RING * (RING + (z + j) % RING) + x, 1), :]
                    scaled[slot, at, i * part : (i + 1) * part] = (piece * row).astype(BF16)
                high, low = two_parts(squares)
                high = jnp.broadcast_to(high.astype(F32), (half, LANES))
                low = jnp.broadcast_to(low.astype(F32), (half, LANES))
                parts[slot, at] = jnp.where(lane == 0, high, jnp.where(lane == 1, low, 0.0))
        copy.wait()

        def run(at, value_at):
            gate_out[:, at] = up_dot(scaled[0], weights, last, at).astype(BF16)
            value_out[:, at] = up_dot(scaled[0], weights, last, value_at).astype(BF16)

        over_tiles(run, 2)
        gate_out[:, inner:] = parts[0, :, :spare].astype(BF16)

    up_flops = 2 * length * span * inner
    gate_shape, value_shape = (length, padded), (length, inner)
    gate_two, value_two, scaled, parts, last = kernel_call(
        up_far_body,
        [
            (gate_shape, BF16),
            (value_shape, BF16),
            ((RING, length, span), BF16),
            ((RING, length, LANES), F32),
            ((2 * inner, part), BF16),
        ],
        flops=2 * up_flops,
        scratch=[pltpu.SemaphoreType.DMA((1,))],
        hbm_in=range(4, 5),
        limit=24,
    )(mine, theirs, gains, weights, ups[3])
    gate_two = shift_x(gate_two, 1)
    value_two = shift_x(value_two, -1)

    def up_near_body(scaled, parts, weights, last, *outs):
        gate_out, value_out, gate_add, value_add, gate_own, value_own = outs
        left = scaled[1:RING].reshape((RING - 1) * length, span)

        def run(at, value_at):
            piece = up_dot(left, weights, last, at)
            gate_out[:, at] = piece[:length].astype(BF16)
            gate_add[:, at] = piece[length : 2 * length]
            gate_own[:, at] = piece[2 * length :]
            piece = up_dot(left, weights, last, value_at)
            value_add[:, at] = piece[:length]
            value_out[:, at] = piece[length : 2 * length].astype(BF16)
            value_own[:, at] = piece[2 * length :]

        over_tiles(run)
        gate_out[:, inner:] = parts[1, :, :spare].astype(BF16)
        gate_add[:, inner:] = parts[2, :, :spare]
        gate_own[:, inner:] = parts[3, :, :spare]

    gate_near, value_near, gate_add, value_add, gate_own, value_own = kernel_call(
        up_near_body,
        [(gate_shape, BF16), (value_shape, BF16)] + [(gate_shape, F32), (value_shape, F32)] * 2,
        flops=6 * up_flops,
        limit=24,
    )(scaled, parts, weights, last)
    gate_near = shift_x(gate_near, -1)
    value_near = shift_x(value_near, 1)

    def up_join_body(gate_two, value_two, gate_add, value_add, gate_out, value_out):
        def step(n, carry):
            at = aligned(n * 16, 16)
            gate_out[at] = (gate_two[at].astype(F32) + gate_add[at]).astype(BF16)
            value_out[at] = (value_two[at].astype(F32) + value_add[at]).astype(BF16)
            return carry

        lax.fori_loop(0, length // 16, step, 0)
        total = gate_two[:, inner:].astype(F32) + gate_add[:, inner:]
        high, low = two_parts(total[:, 0:1] + total[:, 1:2])
        gate_out[:, inner : inner + 1] = high
        gate_out[:, inner + 1 : inner + 2] = low

    gate_join, value_join = kernel_call(
        up_join_body, [(gate_shape, BF16), (value_shape, BF16)]
    )(gate_two, value_two, gate_add, value_add)
    gate_join = shift_x(gate_join, 1)
    value_join = shift_x(value_join, -1)

    def active_body(
        gate_own, gate_near, gate_join, value_own, value_near, value_join,
        gate_kernel, value_kernel, gate_offset, value_offset, out,
    ):
        gates, values = (gate_own, gate_near, gate_join), (value_own, value_near, value_join)
        squares = jnp.zeros((length, 1), F32)
        for ref in gates:
            squares = squares + ref[:, inner : inner + 1].astype(F32)
            squares = squares + ref[:, inner + 1 : inner + 2].astype(F32)
        scale = lax.rsqrt(squares / full + epsilon)

        def run(at, size):
            position = lax.broadcasted_iota(jnp.int32, (length, size), 0)

            def convolve(refs, kernel, offset):
                total = refs[0][:, at] + refs[1][:, at].astype(F32) + refs[2][:, at].astype(F32)
                pre = (total * scale).astype(BF16).astype(F32)
                before = jnp.where(position == 0, 0.0, pltpu.roll(pre, 1, 0))
                after = jnp.where(position == length - 1, 0.0, pltpu.roll(pre, length - 1, 0))
                taps = before * kernel[0:1, at] + pre * kernel[1:2, at] + after * kernel[2:3, at]
                return offset[:, at] + taps

            gate = convolve(gates, gate_kernel, gate_offset)
            value = convolve(values, value_kernel, value_offset)
            out[:, at] = (gelu_exact(gate) * value).astype(BF16)

        def step(n, carry):
            run(aligned(n * LANES, LANES), LANES)
            return carry

        lax.fori_loop(0, inner // LANES, step, 0, unroll=2)
        rest = inner // LANES * LANES
        run(slice(rest, inner), inner - rest)

    (active,) = kernel_call(active_body, [((length, inner), BF16)], flops=1 << 24)(
        gate_own, gate_near, gate_join, value_own, value_near, value_join,
        gate_kernel, value_kernel, gate_offset[None], value_offset[None],
    )
    actives = gather_ring(active, (X,), RING)

    def down_load_body(*refs):
        order = order_z(place()[3])
        move(*((refs[i], refs[RING].at[j]) for i, j in enumerate(order)), refs[RING + 1])

    (weights,) = kernel_call(
        down_load_body,
        [((RING, inner, part), BF16)],
        scratch=[load_sems],
        hbm_in=range(4),
    )(*downs)


    def down_body(side_is_own):
        def run(*refs):
            actives, weights, out, blocks, left = refs[0:4], refs[4], refs[5], refs[6], refs[7]
            _, x, _, core = place()
            side = core if side_is_own else 1 - core
            left[...] = side_of(actives, order_before(core), blocks, x, side)

            def step(j, carry):
                out[j] = dot(left[...], weights[j]).astype(out.dtype)
                return carry

            lax.fori_loop(0, RING, step, 0, unroll=True)

        return kernel_call(
            run,
            [((RING, own_rows, part), F32 if side_is_own else BF16)],
            flops=2 * own_rows * inner * span,
            scratch=[pltpu.VMEM((RING, length, inner), BF16), pltpu.VMEM((own_rows, inner), BF16)],
        )

    (other,) = down_body(False)(*actives, weights)
    received = swap_core(other)
    (own,) = down_body(True)(*actives, weights)

    def down_add_body(*refs):
        own, received, mine, keep, sends = refs[0], refs[1], refs[2], refs[3], refs[4:7]
        z, _, y, _ = place()
        at = (y - z) % RING
        for k in range(1, RING):
            j = (at + k) % RING
            sends[k - 1][...] = (own[j] + received[j].astype(F32)).astype(BF16)
        keep[...] = own[at] + received[at].astype(F32)
        for k in range(RING):
            place_rows = aligned(half * ((y - k) % RING), half)
            for j in range(RING):

                @pl.when(at == j)
                def _():
                    piece = mine[k, :, j * part : (j + 1) * part].astype(F32)
                    keep[place_rows, :] = keep[place_rows, :] + piece

    block = (own_rows, part)
    keep, *sends = kernel_call(
        down_add_body, [(block, F32)] + [(block, BF16)] * 3, flops=1 << 20
    )(own, received, mine)
    sums = [shift_y(sends[k - 1], k) for k in range(1, RING)]

    def result_body(keep, first, second, third, near, far, total):
        x = place()[1]
        added = keep[...] + first[...].astype(F32) + second[...].astype(F32)
        total[...] = added + third[...].astype(F32)
        near[...] = total[aligned(length * (x % 2), length), :].astype(BF16)
        far[...] = total[aligned(length * (1 - x % 2), length), :].astype(BF16)

    near, far = kernel_call(
        result_body, [piece, piece], scratch=[pltpu.VMEM(block, F32)]
    )(keep, *sums)

    near, far = trade(near, False), trade(far, True)

    def exit_body(near, far, out, sems):
        x = place()[1]
        move(
            (near, out.at[:, aligned(part * (x % 2), part)]),
            (far, out.at[:, aligned(part * (1 - x % 2), part)]),
            sems,
        )

    (out,) = kernel_call(
        exit_body,
        [((length, features), BF16)],
        scratch=[pltpu.SemaphoreType.DMA((2,))],
        hbm_in=range(2),
        hbm_out=range(1),
    )(near, far)
    return out


def solution(mesh):
    finer = Mesh(
        mesh.devices.reshape(mesh.shape["rep"], RING, RING, RING, 2), (REP, ZLO, X, Y, CORE)
    )

    return jax.shard_map(
        body,
        mesh=finer,
        in_specs=(
            P(REP_FS, TP),
            P(),
            P(FS, TP),
            P(FS, TP),
            P(TP, None),
            P(TP, FS, None),
            P(TP, None),
            P(TP, None),
            P(TP, FS),
            P(),
            P(FS, TP),
            P(FS, TP),
            P(None, TP),
            P(None, TP),
            P(TP),
            P(TP),
            P(TP, FS),
        ),
        out_specs=P(REP_FS, TP),
        check_vma=False,
    )
```
